32 devices in a mesh: ep: 8 (over z, x), tp: 4 (over y, core).
Axes of the slice: x: 2, y: 2, z: 4, core: 2. Of those that a mesh axis runs over, the one named last changes fastest.
Arguments:
- receptance: bfloat16 [4096, 1024], P('ep', 'tp'), may hold values from -6 to 6
- key_matrix: bfloat16 [4096, 1024], P('ep', 'tp'), may hold values from -6 to 6
- value_matrix: bfloat16 [4096, 1024], P('ep', 'tp'), may hold values from -6 to 6
- decay_data_term: bfloat16 [4096, 1024], P('ep', 'tp'), may hold values from -3.5 to 3.5
- correction_rate_data: bfloat16 [4096, 1024], P('ep', 'tp'), may hold values from -6 to 6
- output_gate_input: bfloat16 [4096, 1024], P('ep', 'tp'), may hold values from -6 to 6
- decay_channel_offset: float32 [1024], P('tp'), may hold values from -12 to -2
- correction_rate_offset: float32 [1024], P('tp'), may hold values from -12 to 1
- extra_head_log_decay: float32 [4096, 16], P('ep', 'tp'), may hold values from -2.1 to 0, as said below
- head_norm_gain: float32 [1024], P('tp'), may hold values from 0.1 to 1.9
- mixer_output_weight: bfloat16 [1024, 2048], P('tp'), may hold values from -0.1875 to 0.1875
- expert_layer_input: bfloat16 [1024, 2048], P('ep'), may hold values from -6 to 6
- feedforward_norm_gain: float32 [2048], replicated, may hold values from 0.1 to 1.9
- group_router_weight: bfloat16 [2048, 4], replicated, may hold values from -0.125 to 0.125
- expert_router_weight: bfloat16 [2048, 8], replicated, may hold values from -0.125 to 0.125
- routes: int32 [1024, 2], P('ep'), may hold values from 0 to 7, all different within a row; in each aligned block of 128 rows (0 to 127, 128 to 255, ...) at most 64 rows name the same one
- expert_gate_weight: bfloat16 [8, 2048, 4096], P('ep', None, 'tp'), may hold values from -0.125 to 0.125
- expert_up_weight: bfloat16 [8, 2048, 4096], P('ep', None, 'tp'), may hold values from -0.125 to 0.125
- expert_down_weight: bfloat16 [8, 4096, 2048], P('ep', 'tp'), may hold values from -0.09375 to 0.09375
Outputs:
- token_mixer_output: bfloat16 [4096, 2048], P(('ep', 'tp'))
- expert_out: bfloat16 [1024, 2048], P('ep', 'tp')
The draws below stay inside these ranges and needn't reach their ends.
Inputs may be any that keep to these rules, and one draw needn't show every extreme that they name: A token's routes are distinct. Within the rows of one index of ep, no expert is named by more than 64 rows, a bound that some block reaches. `extra_head_log_decay`: entries are zero or negative; each head has a few nonzero positions.
All inputs are finite; a program needn't handle non-finite values.
Results may differ from the reference program's by a relative error of at most 0.022.
Values may be sent and summed in bfloat16 or wider, within the bound.
A program may use at most 128 MiB of HBM per device.

```python
import math
import jax
import jax.numpy as jnp
import numpy as np
from jax import lax

D = 2048
HEAD_DIM = 64
HEADS = 16
MIX = 1024
FF = 4096
GROUPS = 4
EXPERTS = 8
TOP = 2
MIX_ROWS = 512
MIX_TOKENS = 4096
MOE_ROWS = 128
MOE_TOKENS = 1024
CAP = 64
N_EP = 8
N_TP = 4


def slow_heads(key):
    share = 0.5
    return jax.random.uniform(jax.random.fold_in(key, 101), (HEADS,)) < share


def draw_decay_channel_offset(key, part):
    slow = slow_heads(key)
    slow_level = math.log(0.5 / MIX_TOKENS) + 0.5
    fast_level = math.log(0.03) + 0.5
    level = jnp.where(slow, slow_level, fast_level)
    jitter = jax.random.uniform(jax.random.fold_in(key, 3), (HEADS, HEAD_DIM), jnp.float32, -0.3, 0.3)
    return (level[:, None] + jitter).reshape(MIX).astype(jnp.float32)


def draw_correction_rate_offset(key, part):
    slow = slow_heads(key)
    slow_level = math.log(6.0 / MIX_TOKENS)
    spread = jax.random.uniform(jax.random.fold_in(key, 5), (HEADS, HEAD_DIM), jnp.float32, -1.0, 1.0)
    level = jnp.where(slow[:, None], slow_level + 0.3 * spread, spread)
    return level.reshape(MIX).astype(jnp.float32)


def draw_decay_data_term(key, part):
    blocks = MIX_TOKENS // MIX_ROWS
    offset = jax.random.uniform(jax.random.fold_in(key, 7), (blocks, 1, HEADS, 1), jnp.float32, -0.4, 0.4)
    noise = 0.5 * jax.random.normal(jax.random.fold_in(key, 9), (blocks, MIX_ROWS, HEADS, HEAD_DIM), jnp.float32)
    return (offset + noise).reshape(MIX_TOKENS, MIX).astype(jnp.bfloat16)


def draw_extra_head_log_decay(key, part):
    where_at = jax.random.randint(jax.random.fold_in(key, 13), (3, HEADS), 0, MIX_TOKENS)
    depth = jnp.log(jax.random.uniform(jax.random.fold_in(key, 17), (3, HEADS), jnp.float32, 0.5, 0.8))
    positions = jnp.arange(MIX_TOKENS)[:, None, None]
    struck = positions == where_at[None, :, :]
    return jnp.sum(jnp.where(struck, depth[None, :, :], 0.0), axis=1).astype(jnp.float32)


def levels(rng, extent, shards, low, high):
    loudness, own = 1.0, jax.random.fold_in(rng, 6)
    for position, blocks in shards:
        draws = jnp.exp(jax.random.uniform(jax.random.fold_in(own, position), (blocks,), jnp.float32, low / len(shards), high / len(shards)))
        loudness = loudness * jnp.repeat(draws, extent[position] // blocks).reshape([-1 if axis == position else 1 for axis in range(len(extent))])
    return loudness


def routed_block(own_key, own, number, rows, count, top, reach, skew):
    sequence = jax.random.permutation(own_key, count)
    heavy_load, ordinary = shares(count, rows * top, reach, skew, True), shares(count, rows * top, reach, skew, False)
    places = jnp.arange(count)

    def named(tallies, offset_by):
        used = int((tallies > 0).sum())
        fixed = max(1, used // 4)
        shifted = fixed + (places - fixed + offset_by * (used - fixed)) % max(1, count - fixed)
        return jnp.zeros((count,), jnp.int32).at[sequence[jnp.where(places < fixed, places, shifted)]].set(jnp.asarray(tallies, jnp.int32))

    tallies = jnp.where(number % 4 == 0, named(heavy_load, number // 4), named(ordinary, number - number // 4 - 1))
    mixed = jax.random.permutation(jax.random.fold_in(own, 3), count)
    giver, sink = mixed[0:count // 2 * 2:2], mixed[1:count // 2 * 2:2]
    margin = jnp.minimum(tallies[giver] - 1, reach - tallies[sink]) // 2
    margin = jnp.where((giver == sequence[0]) | (sink == sequence[0]) | (tallies[sink] == 0), 0, jnp.maximum(margin, 0))
    shifted = jax.random.randint(jax.random.fold_in(own, 4), (count // 2,), 0, 1 << 20) % (margin + 1)
    tallies = tallies.at[giver].add(-shifted).at[sink].add(shifted)
    labels = jnp.searchsorted(jnp.cumsum(tallies), jnp.arange(rows * top), side="right").astype(jnp.int32)
    table = labels.reshape(top, rows).T
    table = table[jax.random.permutation(jax.random.fold_in(own, 1), rows)]
    offset_by = jax.random.randint(jax.random.fold_in(own, 2), (rows, 1), 0, top)
    return jnp.take_along_axis(table, (jnp.arange(top)[None, :] + offset_by) % top, axis=1)


def shares(amount, total, bound, lean, full):
    portions = [(1 << 20) // math.isqrt(standing ** lean) + 1 for standing in range(1, amount + 1)]
    largest = bound if full else min(bound, max(-(-total // amount), total * portions[0] // sum(portions)))
    least = 1 if total - largest >= amount - 1 else 0
    counts, surplus = [largest] + [least] * (amount - 1), total - largest - least * (amount - 1)
    while surplus > 0:
        movable = [i for i in range(1, amount) if counts[i] < largest] or [i for i in range(1, amount) if counts[i] < bound]
        pool, remaining = sum([portions[i] for i in movable]), surplus
        for i in movable:
            addition = min(bound - counts[i], max(1, remaining * portions[i] // pool), surplus)
            counts[i] = counts[i] + addition
            surplus = surplus - addition
    return np.array(counts)


def centred(key, shape, scale, reach, pieces=(), held_as=jnp.bfloat16):
    drawn = scale * jax.random.normal(key, shape, jnp.float32)
    if pieces:
        drawn = drawn * levels(key, shape, pieces, -0.22, 0.18)
    return jnp.clip(drawn, -reach, reach).astype(held_as)


def setup_inputs(seed: int = 0) -> dict:
    splits = jax.random.split(jax.random.key(seed), 20)
    receptance = centred(splits[0], (MIX_TOKENS, MIX), 1.0, 6.0, ((0, 8), (1, 4)))
    key_matrix = centred(splits[1], (MIX_TOKENS, MIX), 1.0, 6.0, ((0, 8), (1, 4)))
    value_matrix = centred(splits[2], (MIX_TOKENS, MIX), 1.0, 6.0, ((0, 8), (1, 4)))
    decay_data_term = draw_decay_data_term(jax.random.fold_in(splits[19], 71), 0)
    correction_rate_data = centred(splits[4], (MIX_TOKENS, MIX), 1.0, 6.0, ((0, 8), (1, 4)))
    output_gate_input = centred(splits[5], (MIX_TOKENS, MIX), 1.0, 6.0, ((0, 8), (1, 4)))
    decay_channel_offset = draw_decay_channel_offset(jax.random.fold_in(splits[19], 71), 0)
    correction_rate_offset = draw_correction_rate_offset(jax.random.fold_in(splits[19], 71), 0)
    extra_head_log_decay = draw_extra_head_log_decay(jax.random.fold_in(splits[19], 71), 0)
    head_norm_gain = jnp.clip(1.0 + 0.18 * jax.random.normal(splits[9], (MIX,), jnp.float32), 0.1, 1.9)
    mixer_output_weight = centred(splits[10], (MIX, D), MIX ** -0.5, 0.1875, ((0, 4),))
    expert_layer_input = centred(splits[11], (MOE_TOKENS, D), 1.0, 6.0, ((0, 8),))
    feedforward_norm_gain = jnp.clip(1.0 + 0.18 * jax.random.normal(splits[12], (D,), jnp.float32), 0.1, 1.9)
    group_router_weight = centred(splits[13], (D, GROUPS), D ** -0.5, 0.125)
    expert_router_weight = centred(splits[14], (D, EXPERTS), D ** -0.5, 0.125)
    routes_keys = jax.random.split(jax.random.fold_in(splits[15], 1), MOE_TOKENS // MOE_ROWS)
    routes_turns = jax.random.permutation(jax.random.fold_in(splits[15], 3), MOE_TOKENS // MOE_ROWS)
    routes = jax.vmap(lambda own, number: routed_block(jax.random.fold_in(splits[15], 2), own, number, MOE_ROWS, EXPERTS, TOP, CAP, 2))(routes_keys, routes_turns).reshape((MOE_TOKENS, TOP))
    expert_gate_weight = centred(splits[16], (EXPERTS, D, FF), D ** -0.5, 0.125, ((0, 8), (2, 4)))
    expert_up_weight = centred(splits[17], (EXPERTS, D, FF), D ** -0.5, 0.125, ((0, 8), (2, 4)))
    expert_down_weight = centred(splits[18], (EXPERTS, FF, D), FF ** -0.5, 0.09375, ((0, 8), (1, 4)))
    return {"receptance": receptance, "key_matrix": key_matrix, "value_matrix": value_matrix, "decay_data_term": decay_data_term, "correction_rate_data": correction_rate_data, "output_gate_input": output_gate_input, "decay_channel_offset": decay_channel_offset, "correction_rate_offset": correction_rate_offset, "extra_head_log_decay": extra_head_log_decay, "head_norm_gain": head_norm_gain, "mixer_output_weight": mixer_output_weight, "expert_layer_input": expert_layer_input, "feedforward_norm_gain": feedforward_norm_gain, "group_router_weight": group_router_weight, "expert_router_weight": expert_router_weight, "routes": routes, "expert_gate_weight": expert_gate_weight, "expert_up_weight": expert_up_weight, "expert_down_weight": expert_down_weight}


key_eps = 1e-06
group_eps = 0.00064
norm_eps = 1e-06
highest = lax.Precision.HIGHEST

def token_mixer_block(receptance, key_matrix, value_matrix, decay_data_term, correction_rate_data, output_gate_input, decay_channel_offset, correction_rate_offset, extra_head_log_decay, head_norm_gain, mixer_output_weight):
    positions = receptance.shape[0]

    def head_view(tensor_in):
        return tensor_in.astype(jnp.float32).reshape(positions, HEADS, HEAD_DIM)
    recept = head_view(receptance)
    keyed = head_view(key_matrix)
    valued = head_view(value_matrix)
    unit_keys = keyed * lax.rsqrt(lax.optimization_barrier(jnp.sum(keyed * keyed, axis=-1, keepdims=True)) + key_eps)
    learn_rate = jax.nn.sigmoid(head_view(correction_rate_data) + correction_rate_offset.reshape(HEADS, HEAD_DIM))
    decay_preactivation = head_view(decay_data_term) + decay_channel_offset.reshape(HEADS, HEAD_DIM)
    decay_factor = jnp.exp(-jnp.exp(-jax.nn.softplus(-decay_preactivation) - 0.5) + extra_head_log_decay[:, :, None])
    removal = unit_keys * learn_rate

    def advance(state, inputs):
        recept_now, decay_now, unit_now, removal_now, key_now, value_now = inputs
        along = jnp.einsum('hvk,hk->hv', state, unit_now, precision=highest)
        state = state * decay_now[:, None, :] - along[:, :, None] * removal_now[:, None, :] + value_now[:, :, None] * key_now[:, None, :]
        return (state, jnp.einsum('hvk,hk->hv', state, recept_now, precision=highest))
    start_state = jnp.zeros((HEADS, HEAD_DIM, HEAD_DIM), jnp.float32)
    _, head_out = lax.scan(advance, start_state, (recept, decay_factor, unit_keys, removal, keyed, valued))
    centre = lax.optimization_barrier(jnp.mean(head_out, axis=-1, keepdims=True))
    spread = lax.optimization_barrier(jnp.mean(jnp.square(head_out - centre), axis=-1, keepdims=True))
    normed = (head_out - centre) * lax.rsqrt(spread + group_eps)
    gated = normed * head_norm_gain.reshape(HEADS, HEAD_DIM) * jax.nn.sigmoid(head_view(output_gate_input))
    mixed_hidden = gated.reshape(positions, MIX).astype(jnp.bfloat16)
    hidden_groups = jnp.moveaxis(mixed_hidden.reshape(positions, N_TP, MIX // N_TP), 1, 0)
    weight_groups = mixer_output_weight.reshape(N_TP, MIX // N_TP, D)

    def add_group(total, pair):
        block_hidden, block_weight = pair
        part = jnp.dot(block_hidden, block_weight, preferred_element_type=jnp.float32).astype(jnp.bfloat16)
        part = lax.optimization_barrier(part)
        return (total + part.astype(jnp.float32), None)
    total, _ = lax.scan(add_group, jnp.zeros((positions, D), jnp.float32), (hidden_groups, weight_groups))
    return total.astype(jnp.bfloat16)

def expert_block(expert_layer_input, feedforward_norm_gain, group_router_weight, expert_router_weight, routes, expert_gate_weight, expert_up_weight, expert_down_weight):
    tokens = expert_layer_input.shape[0]
    widened = expert_layer_input.astype(jnp.float32)
    normed_input = (widened * lax.rsqrt(lax.optimization_barrier(jnp.mean(widened * widened, axis=-1, keepdims=True)) + norm_eps) * feedforward_norm_gain).astype(jnp.bfloat16)
    group_logit = jnp.dot(normed_input, group_router_weight, preferred_element_type=jnp.float32)
    group_exp = jnp.exp(group_logit)
    group_prob = group_exp / lax.optimization_barrier(jnp.sum(group_exp, axis=-1, keepdims=True))
    expert_logit = jnp.dot(normed_input, expert_router_weight, preferred_element_type=jnp.float32)
    per_group = EXPERTS // GROUPS
    chosen_logit = jnp.take_along_axis(expert_logit, routes, axis=1)
    chosen_group = jnp.take_along_axis(group_prob, routes // per_group, axis=1)
    route_weight = chosen_group * jax.nn.sigmoid(chosen_logit - chosen_logit[:, ::-1])
    flat_routes = routes.reshape(-1)
    onehot = (flat_routes[:, None] == jnp.arange(EXPERTS, dtype=jnp.int32)[None, :]).astype(jnp.int32)
    ranked = lax.optimization_barrier(jnp.sum((jnp.cumsum(onehot, axis=0) - onehot) * onehot, axis=1))
    room = N_EP * CAP
    destination = (flat_routes * room + ranked).astype(jnp.int32)
    source_rows = jnp.zeros((EXPERTS * room,), jnp.int32).at[destination].set((jnp.arange(flat_routes.shape[0], dtype=jnp.int32) // TOP).astype(jnp.int32))
    gathered = normed_input[source_rows].reshape(EXPERTS, room, D)

    def run_expert(pack):
        rows_in, gate_mat, up_mat, down_mat = pack
        gate_val = jnp.dot(rows_in, gate_mat, preferred_element_type=jnp.float32)
        up_val = jnp.dot(rows_in, up_mat, preferred_element_type=jnp.float32)
        expert_hidden = (jax.nn.silu(gate_val) * up_val).astype(jnp.bfloat16)
        hidden_groups = expert_hidden.reshape(room, N_TP, FF // N_TP)
        down_groups = down_mat.reshape(N_TP, FF // N_TP, D)
        total = jnp.zeros((room, D), jnp.float32)
        for member in range(N_TP):
            part = jnp.dot(hidden_groups[:, member], down_groups[member], preferred_element_type=jnp.float32).astype(jnp.bfloat16)
            part = lax.optimization_barrier(part)
            total = total + part.astype(jnp.float32)
        return total.astype(jnp.bfloat16)
    expert_rows = lax.map(run_expert, (gathered, expert_gate_weight, expert_up_weight, expert_down_weight)).reshape(EXPERTS * room, D)
    picked = expert_rows[destination].astype(jnp.float32).reshape(tokens, TOP, D)
    return lax.optimization_barrier(jnp.sum(picked * route_weight[:, :, None], axis=1)).astype(jnp.bfloat16)

def reference(receptance, key_matrix, value_matrix, decay_data_term, correction_rate_data, output_gate_input, decay_channel_offset, correction_rate_offset, extra_head_log_decay, head_norm_gain, mixer_output_weight, expert_layer_input, feedforward_norm_gain, group_router_weight, expert_router_weight, routes, expert_gate_weight, expert_up_weight, expert_down_weight):
    token_mixer_output = token_mixer_block(receptance, key_matrix, value_matrix, decay_data_term, correction_rate_data, output_gate_input, decay_channel_offset, correction_rate_offset, extra_head_log_decay, head_norm_gain, mixer_output_weight)
    expert_out = expert_block(expert_layer_input, feedforward_norm_gain, group_router_weight, expert_router_weight, routes, expert_gate_weight, expert_up_weight, expert_down_weight)
    return (token_mixer_output, expert_out)
```

```python
import functools
import math

import jax
import jax.numpy as jnp
from jax import lax
from jax.experimental import pallas as pl
from jax.experimental.pallas import tpu as pltpu
from jax.sharding import PartitionSpec as P

HEAD_DIM = 64
PAIR = 2 * HEAD_DIM
HALF_EXP = math.exp(-0.5)
GROUPS = 4


key_eps = 1e-06
group_eps = 0.00064
norm_eps = 1e-06
highest = lax.Precision.HIGHEST


def bf(x):
    return x.astype(jnp.bfloat16)


def mm(x, y):
    return lax.dot_general(x, y, (((1,), (0,)), ((), ())), preferred_element_type=jnp.float32)


def mm_nt(x, y):
    return lax.dot_general(x, y, (((1,), (1,)), ((), ())), preferred_element_type=jnp.float32)


def mm_tn(x, y):
    return lax.dot_general(x, y, (((0,), (0,)), ((), ())), preferred_element_type=jnp.float32)


def halves(x):
    high = bf(x)
    return high, bf(x - high.astype(jnp.float32))


def sum_right(x, ones):
    high, low = halves(x)
    return mm(high, ones) + mm(low, ones)


def logistic(x):
    return 1.0 / (1.0 + jnp.exp(-x))


def flag(cond):
    return jnp.where(cond, 1.0, 0.0)


def iota(shape, dim):
    return lax.broadcasted_iota(jnp.int32, shape, dim)


def pair_blocks():
    return flag((iota((PAIR, PAIR), 0) < HEAD_DIM) == (iota((PAIR, PAIR), 1) < HEAD_DIM))


def scan_kernel(
    group,
    r_ref,
    k_ref,
    v_ref,
    d_ref,
    a_ref,
    d_off_ref,
    a_off_ref,
    extra_ref,
    out_ref,
    reach_ref,
    ends_ref,
    chain_ref,
):
    positions, width = r_ref.shape
    pairs = width // PAIR
    C = HEAD_DIM
    rows_per = group * C
    own_block = pair_blocks()
    own_bf = bf(own_block)
    row, col = iota((C, PAIR), 0), iota((C, PAIR), 1) & (HEAD_DIM - 1)
    strict, upto = row > col, row >= col
    eye = flag(row == col)
    first = iota((1, PAIR), 1) < HEAD_DIM
    tri = bf(flag(iota((C, C), 0) >= iota((C, C), 1)))
    level_masks = []
    for s in range(6):
        inside = (
            ((row >> (s + 1)) == (col >> (s + 1)))
            & (((row >> s) & 1) == 1)
            & (((col >> s) & 1) == 0)
        )
        level_masks.append(bf(flag(inside)))

    def spread(x):
        return jnp.concatenate([x, x], axis=0) * own_bf

    square = (iota((PAIR, PAIR), 0) == iota((PAIR, PAIR), 1)).astype(jnp.float32)
    for p in range(pairs):
        chain_ref[p, :PAIR] = jnp.zeros((PAIR, PAIR), jnp.float32)
        chain_ref[p, PAIR:] = square

    def step(g, carry):
        base = pl.multiple_of(g * rows_per, rows_per)
        rows = pl.ds(base, rows_per)
        items = []
        for p in range(pairs):
            lanes = slice(p * PAIR, (p + 1) * PAIR)
            k = k_ref[rows, lanes].astype(jnp.float32)
            u = k * lax.rsqrt(sum_right(k * k, own_bf) + key_eps)
            rem = u * logistic(a_ref[rows, lanes].astype(jnp.float32) + a_off_ref[:, lanes])
            e = extra_ref[rows, :]
            extra = jnp.where(first, e[:, 2 * p : 2 * p + 1], e[:, 2 * p + 1 : 2 * p + 2])
            lg = extra - HALF_EXP * logistic(
                d_ref[rows, lanes].astype(jnp.float32) + d_off_ref[:, lanes]
            )
            r = r_ref[rows, lanes].astype(jnp.float32)
            v = v_ref[rows, lanes]
            for c in range(group):
                cut = slice(c * C, (c + 1) * C)
                items.append((p, c, k[cut], u[cut], rem[cut], lg[cut], r[cut], v[cut]))
        stage = []
        for p, c, k, u, rem, lg, r, v in items:
            high, low = halves(lg)
            rest = bf(lg - high.astype(jnp.float32) - low.astype(jnp.float32))
            cumul = mm(tri, high) + mm(tri, low) + mm(tri, rest)
            stage.append(cumul)
        work = []
        for (p, c, k, u, rem, lg, r, v), cumul in zip(items, stage):
            mid = 0.5 * cumul[C - 1 : C]
            up_now, down = jnp.exp(cumul - mid), jnp.exp(mid - cumul)
            up_before = jnp.exp(cumul - lg - mid)
            half = jnp.exp(mid)
            cq, cu, dk, dr = r * up_now, u * up_before, k * down, rem * down
            left = bf(jnp.concatenate([cu, cq], axis=0))
            pair_r = mm_nt(left, spread(bf(dr)))
            pair_k = mm_nt(left, spread(bf(dk)))
            work.append((cq * half, bf(cu * half), bf(dk * half), bf(dr * half), half * half, pair_r, pair_k))
        solve = []
        for (p, c, k, u, rem, lg, r, v), (qe, ue, kt, rt, ed, pair_r, pair_k) in zip(items, work):
            rp = bf(jnp.where(strict, pair_r[:C], 0.0))
            rr = bf(jnp.where(upto, pair_r[C:], 0.0))
            kp = jnp.where(strict, pair_k[:C], 0.0)
            rk = jnp.where(upto, pair_k[C:], 0.0)
            kv = mm(bf(jnp.concatenate([kp, rk], axis=0)), spread(v))
            inv = eye - (rp * level_masks[0]).astype(jnp.float32)
            solve.append([rp, rr, kv, inv])
        for s in range(1, 6):
            mids = [bf(mm(bf(inv), spread(rp * level_masks[s]))) for rp, rr, kv, inv in solve]
            for item, y in zip(solve, mids):
                item[3] = item[3] - mm(y, spread(bf(item[3])))
        wvs = []
        for (rp, rr, kv, inv), w in zip(solve, work):
            wide = jnp.concatenate([spread(w[1]), spread(bf(kv[:C]))], axis=1)
            wvs.append(bf(mm(bf(inv), wide)))
        tails = []
        for (rp, rr, kv, inv), (qe, ue, kt, rt, ed, _, _), wv, item in zip(solve, work, wvs, items):
            wide = jnp.concatenate([spread(wv[:, :PAIR]), spread(wv[:, PAIR:])], axis=1)
            rw = mm(rr, wide)
            read = bf(qe - rw[:, :PAIR])
            local = kv[C:] - rw[:, PAIR:]
            v = item[7]
            x = jnp.concatenate(
                [jnp.concatenate([v, jnp.zeros_like(v)], axis=1),
                 jnp.concatenate([-wv[:, PAIR:], -wv[:, :PAIR]], axis=1)], axis=0)
            nb = mm_tn(x, jnp.concatenate([kt, rt], axis=0))
            tails.append((read, local, nb[:PAIR] * own_block, bf(nb[PAIR:] * own_block), ed))
        z = [chain_ref[p] for p in range(pairs)]
        for c in range(group):
            for p in range(pairs):
                read, local, add, neg, ed = tails[p * group + c]
                zb = bf(z[p])
                qz = mm_nt(read, zb)
                at = pl.ds(pl.multiple_of(base + c * C, C), C)
                lanes = slice(p * PAIR, (p + 1) * PAIR)
                out_ref[at, lanes] = local + qz[:, :PAIR]
                reach_ref[at, lanes] = bf(qz[:, PAIR:])
                moved = z[p] * ed + mm(zb, neg)
                z[p] = jnp.concatenate([moved[:PAIR] + add, moved[PAIR:]], axis=0)
        for p in range(pairs):
            chain_ref[p] = z[p]
        return carry

    lax.fori_loop(0, positions // rows_per, step, 0)
    for p in range(pairs):
        s, m = chain_ref[p, :PAIR], chain_ref[p, PAIR:]
        ends_ref[p * 2 * C : p * 2 * C + C] = bf(s[:C] + s[C:])
        ends_ref[p * 2 * C + C : (p + 1) * 2 * C] = bf(m[:C] + m[C:])


def join_kernel(axis, all_ref, out_ref, reach_ref, gate_ref, gain_ref, mixed_ref):
    devices, place = lax.axis_size(axis), lax.axis_index(axis)
    width = out_ref.shape[1]
    pairs = width // PAIR
    C = HEAD_DIM
    own_block = pair_blocks()
    own_bf = bf(own_block)
    mean_bf = bf(own_block * (1.0 / HEAD_DIM))
    states = [jnp.zeros((C, PAIR), jnp.float32) for _ in range(pairs)]

    def hop(j, states):
        new = []
        for p in range(pairs):
            s = all_ref[j, p * 2 * C : p * 2 * C + C].astype(jnp.float32)
            m = all_ref[j, p * 2 * C + C : (p + 1) * 2 * C]
            m = jnp.concatenate([m, m], axis=0) * own_bf
            new.append(sum_right(states[p], m) + s)
        return tuple(new)

    states = lax.fori_loop(0, place, hop, tuple(states))
    for p in range(pairs):
        lanes = slice(p * PAIR, (p + 1) * PAIR)
        s = bf(states[p])
        s = jnp.concatenate([s, s], axis=0) * own_bf
        head = out_ref[:, lanes] + mm_nt(reach_ref[:, lanes], s)
        centred = head - sum_right(head, mean_bf)
        spread = sum_right(centred * centred, mean_bf)
        normed = centred * lax.rsqrt(spread + group_eps)
        gate = logistic(gate_ref[:, lanes].astype(jnp.float32))
        mixed_ref[:, lanes] = bf(normed * gain_ref[:, lanes] * gate)


def mixer_part(
    receptance,
    key_matrix,
    value_matrix,
    decay_data_term,
    correction_rate_data,
    output_gate_input,
    decay_channel_offset,
    correction_rate_offset,
    extra_head_log_decay,
    head_norm_gain,
    mixer_output_weight,
):
    positions, own_width = receptance.shape
    pairs = -(-own_width // PAIR)
    width = pairs * PAIR

    def filled(x, columns=width):
        return x if x.shape[-1] == columns else jnp.pad(x, ((0, 0), (0, columns - x.shape[-1])))

    whole_weight = lax.all_gather(mixer_output_weight, "tp", axis=0, tiled=True)
    blocks = positions // HEAD_DIM
    group = 4 if blocks % 4 == 0 else 1
    local, reach, ends = pl.pallas_call(
        functools.partial(scan_kernel, group),
        out_shape=(
            jax.ShapeDtypeStruct((positions, width), jnp.float32),
            jax.ShapeDtypeStruct((positions, width), jnp.bfloat16),
            jax.ShapeDtypeStruct((pairs * 2 * HEAD_DIM, PAIR), jnp.bfloat16),
        ),
        scratch_shapes=[pltpu.VMEM((pairs, 2 * PAIR, PAIR), jnp.float32)],
        cost_estimate=pl.CostEstimate(
            flops=60000 * positions * width, bytes_accessed=16 * positions * width, transcendentals=0
        ),
    )(
        filled(receptance),
        filled(key_matrix),
        filled(value_matrix),
        filled(decay_data_term),
        filled(correction_rate_data),
        filled(decay_channel_offset[None]),
        filled(correction_rate_offset[None]),
        filled(extra_head_log_decay, 2 * pairs),
    )
    everyone = lax.all_gather(ends, "ep")
    mixed_hidden = pl.pallas_call(
        functools.partial(join_kernel, "ep"),
        out_shape=jax.ShapeDtypeStruct((positions, width), jnp.bfloat16),
        cost_estimate=pl.CostEstimate(
            flops=6000 * positions * width, bytes_accessed=16 * positions * width, transcendentals=0
        ),
    )(everyone, local, reach, filled(output_gate_input), filled(head_norm_gain[None]))
    mixed_hidden = mixed_hidden[:, :own_width]
    own_rows = lax.all_to_all(mixed_hidden, "tp", split_axis=0, concat_axis=1, tiled=True)
    return jnp.dot(own_rows, whole_weight, preferred_element_type=jnp.float32).astype(jnp.bfloat16)


def finish_experts(gate_val, up_val, expert_down_weight):
    expert_hidden = (jax.nn.silu(gate_val) * up_val).astype(jnp.bfloat16)
    return lax.psum_scatter(
        jnp.einsum(
            "sxcf,xfd->dsxc", expert_hidden, expert_down_weight, preferred_element_type=jnp.float32
        ).astype(jnp.bfloat16),
        "tp",
        scatter_dimension=0,
        tiled=True,
    )


def expert_part(
    expert_layer_input,
    feedforward_norm_gain,
    group_router_weight,
    expert_router_weight,
    routes,
    expert_gate_weight,
    expert_up_weight,
    expert_down_weight,
):
    token_rows = expert_layer_input.shape[0]
    route_count = routes.shape[1]
    ep_count = lax.axis_size("ep")
    expert_total = expert_router_weight.shape[1]
    per_group = expert_total // GROUPS
    capacity = 4 * token_rows // ep_count
    widened = expert_layer_input.astype(jnp.float32)
    normed_input = (
        widened
        * lax.rsqrt(jnp.mean(widened * widened, axis=-1, keepdims=True) + norm_eps)
        * feedforward_norm_gain
    ).astype(jnp.bfloat16)
    group_logit = jnp.dot(normed_input, group_router_weight, preferred_element_type=jnp.float32)
    group_exp = jnp.exp(group_logit)
    group_prob = group_exp / jnp.sum(group_exp, axis=-1, keepdims=True)
    expert_logit = jnp.dot(normed_input, expert_router_weight, preferred_element_type=jnp.float32)
    expert_range = jnp.arange(expert_total, dtype=jnp.int32)
    matched = routes[:, :, None] == expert_range[None, None, :]
    chosen_logit = jnp.sum(jnp.where(matched, expert_logit[:, None, :], 0.0), axis=-1)
    group_match = (routes // per_group)[:, :, None] == jnp.arange(GROUPS, dtype=jnp.int32)[
        None, None, :
    ]
    chosen_group = jnp.sum(jnp.where(group_match, group_prob[:, None, :], 0.0), axis=-1)
    route_weight = chosen_group * jax.nn.sigmoid(chosen_logit - chosen_logit[:, ::-1])
    flat_match = matched.reshape(token_rows * route_count, expert_total).astype(jnp.int32)
    before = jnp.cumsum(flat_match, axis=0) - flat_match
    placed = jnp.sum(before * flat_match, axis=1)
    slot_ids = routes.reshape(-1) * capacity + placed
    slot_range = jnp.arange(expert_total * capacity, dtype=jnp.int32)
    struck = (slot_range[:, None] == slot_ids[None, :]).reshape(
        expert_total * capacity, token_rows, route_count
    )
    dispatch_matrix = jnp.any(struck, axis=-1).astype(jnp.bfloat16)
    combine_matrix = jnp.sum(jnp.where(struck, route_weight[None, :, :], 0.0), axis=-1)
    outgoing = jnp.dot(dispatch_matrix, normed_input, preferred_element_type=jnp.float32).astype(
        jnp.bfloat16
    )
    outgoing = outgoing.reshape(ep_count, expert_total // ep_count, capacity, outgoing.shape[1])
    width_share = outgoing.shape[3] // lax.axis_size("tp")
    own_columns = lax.dynamic_slice_in_dim(
        outgoing, lax.axis_index("tp") * width_share, width_share, 3
    )
    piece = lax.all_gather(
        lax.all_to_all(own_columns, "ep", split_axis=0, concat_axis=0, tiled=True),
        "tp",
        axis=3,
        tiled=True,
    )
    gate_val = jnp.einsum(
        "sxcd,xdf->sxcf", piece, expert_gate_weight, preferred_element_type=jnp.float32
    )
    up_val = jnp.einsum(
        "sxcd,xdf->sxcf", piece, expert_up_weight, preferred_element_type=jnp.float32
    )
    expert_rows = finish_experts(gate_val, up_val, expert_down_weight)
    homebound = lax.all_to_all(expert_rows, "ep", split_axis=1, concat_axis=1, tiled=True)
    homebound = homebound.reshape(homebound.shape[0], expert_total * capacity)
    combined = jnp.dot(homebound.astype(jnp.float32), combine_matrix, precision=highest)
    return combined.T.astype(jnp.bfloat16)


def local(
    receptance,
    key_matrix,
    value_matrix,
    decay_data_term,
    correction_rate_data,
    output_gate_input,
    decay_channel_offset,
    correction_rate_offset,
    extra_head_log_decay,
    head_norm_gain,
    mixer_output_weight,
    expert_layer_input,
    feedforward_norm_gain,
    group_router_weight,
    expert_router_weight,
    routes,
    expert_gate_weight,
    expert_up_weight,
    expert_down_weight,
):
    token_mixer_output = mixer_part(
        receptance,
        key_matrix,
        value_matrix,
        decay_data_term,
        correction_rate_data,
        output_gate_input,
        decay_channel_offset,
        correction_rate_offset,
        extra_head_log_decay,
        head_norm_gain,
        mixer_output_weight,
    )
    expert_out = expert_part(
        expert_layer_input,
        feedforward_norm_gain,
        group_router_weight,
        expert_router_weight,
        routes,
        expert_gate_weight,
        expert_up_weight,
        expert_down_weight,
    )
    return (token_mixer_output, expert_out)


def solution(mesh):
    in_specs = (
        P("ep", "tp"),
        P("ep", "tp"),
        P("ep", "tp"),
        P("ep", "tp"),
        P("ep", "tp"),
        P("ep", "tp"),
        P("tp"),
        P("tp"),
        P("ep", "tp"),
        P("tp"),
        P("tp", None),
        P("ep", None),
        P(),
        P(),
        P(),
        P("ep", None),
        P("ep", None, "tp"),
        P("ep", None, "tp"),
        P("ep", "tp", None),
    )
    out_specs = (P(("ep", "tp"), None), P("ep", "tp"))
    return jax.shard_map(local, mesh=mesh, in_specs=in_specs, out_specs=out_specs, check_vma=False)
```

```python
import functools
import math

import jax
import jax.numpy as jnp
from jax import lax
from jax.experimental import pallas as pl
from jax.experimental.pallas import tpu as pltpu
from jax.sharding import PartitionSpec as P

HEAD_DIM = 64
PAIR = 2 * HEAD_DIM
HALF_EXP = math.exp(-0.5)
GROUPS = 4


key_eps = 1e-06
group_eps = 0.00064
norm_eps = 1e-06
highest = lax.Precision.HIGHEST


def bf(x):
    return x.astype(jnp.bfloat16)


def mm(x, y):
    return lax.dot_general(x, y, (((1,), (0,)), ((), ())), preferred_element_type=jnp.float32)


def mm_nt(x, y):
    return lax.dot_general(x, y, (((1,), (1,)), ((), ())), preferred_element_type=jnp.float32)


def mm_tn(x, y):
    return lax.dot_general(x, y, (((0,), (0,)), ((), ())), preferred_element_type=jnp.float32)


def halves(x):
    high = bf(x)
    return high, bf(x - high.astype(jnp.float32))


def sum_right(x, ones):
    high, low = halves(x)
    return mm(high, ones) + mm(low, ones)


def logistic(x):
    return 1.0 / (1.0 + jnp.exp(-x))


def flag(cond):
    return jnp.where(cond, 1.0, 0.0)


def iota(shape, dim):
    return lax.broadcasted_iota(jnp.int32, shape, dim)


def pair_blocks():
    return flag((iota((PAIR, PAIR), 0) < HEAD_DIM) == (iota((PAIR, PAIR), 1) < HEAD_DIM))


def scan_kernel(
    group,
    r_ref,
    k_ref,
    v_ref,
    d_ref,
    a_ref,
    d_off_ref,
    a_off_ref,
    extra_ref,
    out_ref,
    reach_ref,
    ends_ref,
    chain_ref,
):
    positions, width = r_ref.shape
    pairs = width // PAIR
    C = HEAD_DIM
    rows_per = group * C
    own_block = pair_blocks()
    own_bf = bf(own_block)
    row, col = iota((C, PAIR), 0), iota((C, PAIR), 1) & (HEAD_DIM - 1)
    strict, upto = row > col, row >= col
    eye = flag(row == col)
    first = iota((1, PAIR), 1) < HEAD_DIM
    tri = bf(flag(iota((C, C), 0) >= iota((C, C), 1)))
    level_masks = []
    for s in range(6):
        inside = (
            ((row >> (s + 1)) == (col >> (s + 1)))
            & (((row >> s) & 1) == 1)
            & (((col >> s) & 1) == 0)
        )
        level_masks.append(bf(flag(inside)))

    def spread(x):
        return jnp.concatenate([x, x], axis=0) * own_bf

    square = (iota((PAIR, PAIR), 0) == iota((PAIR, PAIR), 1)).astype(jnp.float32)
    for p in range(pairs):
        chain_ref[p, :PAIR] = jnp.zeros((PAIR, PAIR), jnp.float32)
        chain_ref[p, PAIR:] = square

    def step(g, carry):
        base = pl.multiple_of(g * rows_per, rows_per)
        rows = pl.ds(base, rows_per)
        items = []
        for p in range(pairs):
            lanes = slice(p * PAIR, (p + 1) * PAIR)
            k = k_ref[rows, lanes].astype(jnp.float32)
            u = k * lax.rsqrt(sum_right(k * k, own_bf) + key_eps)
            rem = u * logistic(a_ref[rows, lanes].astype(jnp.float32) + a_off_ref[:, lanes])
            e = extra_ref[rows, :]
            extra = jnp.where(first, e[:, 2 * p : 2 * p + 1], e[:, 2 * p + 1 : 2 * p + 2])
            lg = extra - HALF_EXP * logistic(
                d_ref[rows, lanes].astype(jnp.float32) + d_off_ref[:, lanes]
            )
            r = r_ref[rows, lanes].astype(jnp.float32)
            v = v_ref[rows, lanes]
            for c in range(group):
                cut = slice(c * C, (c + 1) * C)
                items.append((p, c, k[cut], u[cut], rem[cut], lg[cut], r[cut], v[cut]))
        stage = []
        for p, c, k, u, rem, lg, r, v in items:
            high, low = halves(lg)
            rest = bf(lg - high.astype(jnp.float32) - low.astype(jnp.float32))
            cumul = mm(tri, high) + mm(tri, low) + mm(tri, rest)
            stage.append(cumul)
        work = []
        for (p, c, k, u, rem, lg, r, v), cumul in zip(items, stage):
            mid = 0.5 * cumul[C - 1 : C]
            up_now, down = jnp.exp(cumul - mid), jnp.exp(mid - cumul)
            up_before = jnp.exp(cumul - lg - mid)
            half = jnp.exp(mid)
            cq, cu, dk, dr = r * up_now, u * up_before, k * down, rem * down
            left = bf(jnp.concatenate([cu, cq], axis=0))
            pair_r = mm_nt(left, spread(bf(dr)))
            pair_k = mm_nt(left, spread(bf(dk)))
            work.append((cq * half, bf(cu * half), bf(dk * half), bf(dr * half), half * half, pair_r, pair_k))
        solve = []
        for (p, c, k, u, rem, lg, r, v), (qe, ue, kt, rt, ed, pair_r, pair_k) in zip(items, work):
            rp = bf(jnp.where(strict, pair_r[:C], 0.0))
            rr = bf(jnp.where(upto, pair_r[C:], 0.0))
            kp = jnp.where(strict, pair_k[:C], 0.0)
            rk = jnp.where(upto, pair_k[C:], 0.0)
            kv = mm(bf(jnp.concatenate([kp, rk], axis=0)), spread(v))
            inv = eye - (rp * level_masks[0]).astype(jnp.float32)
            solve.append([rp, rr, kv, inv])
        for s in range(1, 6):
            mids = [bf(mm(bf(inv), spread(rp * level_masks[s]))) for rp, rr, kv, inv in solve]
            for item, y in zip(solve, mids):
                item[3] = item[3] - mm(y, spread(bf(item[3])))
        wvs = []
        for (rp, rr, kv, inv), w in zip(solve, work):
            wide = jnp.concatenate([spread(w[1]), spread(bf(kv[:C]))], axis=1)
            wvs.append(bf(mm(bf(inv), wide)))
        tails = []
        for (rp, rr, kv, inv), (qe, ue, kt, rt, ed, _, _), wv, item in zip(solve, work, wvs, items):
            wide = jnp.concatenate([spread(wv[:, :PAIR]), spread(wv[:, PAIR:])], axis=1)
            rw = mm(rr, wide)
            read = bf(qe - rw[:, :PAIR])
            local = kv[C:] - rw[:, PAIR:]
            v = item[7]
            x = jnp.concatenate(
                [jnp.concatenate([v, jnp.zeros_like(v)], axis=1),
                 jnp.concatenate([-wv[:, PAIR:], -wv[:, :PAIR]], axis=1)], axis=0)
            nb = mm_tn(x, jnp.concatenate([kt, rt], axis=0))
            tails.append((read, local, nb[:PAIR] * own_block, bf(nb[PAIR:] * own_block), ed))
        z = [chain_ref[p] for p in range(pairs)]
        for c in range(group):
            for p in range(pairs):
                read, local, add, neg, ed = tails[p * group + c]
                zb = bf(z[p])
                qz = mm_nt(read, zb)
                at = pl.ds(pl.multiple_of(base + c * C, C), C)
                lanes = slice(p * PAIR, (p + 1) * PAIR)
                out_ref[at, lanes] = local + qz[:, :PAIR]
                reach_ref[at, lanes] = bf(qz[:, PAIR:])
                moved = z[p] * ed + mm(zb, neg)
                z[p] = jnp.concatenate([moved[:PAIR] + add, moved[PAIR:]], axis=0)
        for p in range(pairs):
            chain_ref[p] = z[p]
        return carry

    lax.fori_loop(0, positions // rows_per, step, 0)
    for p in range(pairs):
        s, m = chain_ref[p, :PAIR], chain_ref[p, PAIR:]
        ends_ref[p * 2 * C : p * 2 * C + C] = bf(s[:C] + s[C:])
        ends_ref[p * 2 * C + C : (p + 1) * 2 * C] = bf(m[:C] + m[C:])


def join_kernel(axis, all_ref, out_ref, reach_ref, gate_ref, gain_ref, mixed_ref):
    devices, place = lax.axis_size(axis), lax.axis_index(axis)
    width = out_ref.shape[1]
    pairs = width // PAIR
    C = HEAD_DIM
    own_block = pair_blocks()
    own_bf = bf(own_block)
    mean_bf = bf(own_block * (1.0 / HEAD_DIM))
    states = [jnp.zeros((C, PAIR), jnp.float32) for _ in range(pairs)]

    def hop(j, states):
        new = []
        for p in range(pairs):
            s = all_ref[j, p * 2 * C : p * 2 * C + C].astype(jnp.float32)
            m = all_ref[j, p * 2 * C + C : (p + 1) * 2 * C]
            m = jnp.concatenate([m, m], axis=0) * own_bf
            new.append(sum_right(states[p], m) + s)
        return tuple(new)

    states = lax.fori_loop(0, place, hop, tuple(states))
    for p in range(pairs):
        lanes = slice(p * PAIR, (p + 1) * PAIR)
        s = bf(states[p])
        s = jnp.concatenate([s, s], axis=0) * own_bf
        head = out_ref[:, lanes] + mm_nt(reach_ref[:, lanes], s)
        centred = head - sum_right(head, mean_bf)
        spread = sum_right(centred * centred, mean_bf)
        normed = centred * lax.rsqrt(spread + group_eps)
        gate = logistic(gate_ref[:, lanes].astype(jnp.float32))
        mixed_ref[:, lanes] = bf(normed * gain_ref[:, lanes] * gate)


def place_of():
    n_ep, n_tp = lax.axis_size("ep"), lax.axis_size("tp")
    e, t = lax.axis_index("ep"), lax.axis_index("tp")
    core = lax.rem(t, 2)
    return n_ep, n_tp, n_tp // 2, e, t, lax.div(t, 2), core


def remote(src, dst, send, recv, e, t):
    return pltpu.make_async_remote_copy(
        src_ref=src,
        dst_ref=dst,
        send_sem=send,
        recv_sem=recv,
        device_id=(e, t),
        device_id_type=pl.DeviceIdType.MESH,
    )


def meet():
    n_ep, n_tp, n_y, e, t, y, core = place_of()
    barrier = pltpu.get_barrier_semaphore()

    def greet(pe, pt):
        pl.semaphore_signal(
            barrier, inc=1, device_id=(pe, pt), device_id_type=pl.DeviceIdType.MESH
        )

    for d in range(1, n_ep):
        greet(lax.rem(e + d, n_ep), t)
    greet(e, 2 * y + 1 - core)
    for d in range(1, n_y):
        greet(e, 2 * lax.rem(y + d, n_y) + core)
    pl.semaphore_wait(barrier, n_ep - 1 + n_y)


def dispatch_kernel(
    cols_ref, ends_ref, piece_ref, every_ref, own_sem, es, er, gs, gr, cs, cr, ys, yr, fs, fr
):
    n_ep, n_tp, n_y, e, t, y, core = place_of()
    share = cols_ref.shape[2]
    other = 2 * y + 1 - core

    def columns(index):
        return pl.ds(pl.multiple_of(index * share, share), share)

    def block(source, index):
        return piece_ref.at[source, :, columns(index)]

    meet()
    own = pltpu.make_async_copy(cols_ref.at[e], block(e, t), own_sem.at[0])
    own_ends = pltpu.make_async_copy(ends_ref, every_ref.at[e], own_sem.at[1])
    own.start()
    own_ends.start()

    def ep_copy(d):
        peer = lax.rem(e + d, n_ep)
        return remote(cols_ref.at[peer], block(e, t), es.at[d], er.at[d], peer, t)

    def ends_copy(d):
        peer = lax.rem(e + d, n_ep)
        return remote(ends_ref, every_ref.at[e], gs.at[d], gr.at[d], peer, t)

    def source(d):
        return lax.rem(e - d + n_ep, n_ep)

    def core_copy(d):
        return remote(block(source(d), t), block(source(d), t), cs.at[d], cr.at[d], e, other)

    def y_copy(d, h):
        peer = 2 * lax.rem(y + h, n_y) + core
        return remote(block(source(d), t), block(source(d), t), ys.at[h, d], yr.at[h, d], e, peer)

    def forward_copy(d, h):
        index = 2 * lax.rem(y - h + n_y, n_y) + core
        return remote(
            block(source(d), index), block(source(d), index), fs.at[h, d], fr.at[h, d], e, other
        )

    def every(first, body):
        def run(d, carry):
            body(d)
            return carry

        lax.fori_loop(first, n_ep, run, 0)

    every(1, lambda d: ep_copy(d).start())
    every(1, lambda d: ends_copy(d).start())

    def share_out(d):
        core_copy(d).start()
        for h in range(1, n_y):
            y_copy(d, h).start()

    own.wait()
    share_out(0)

    def arrived(d):
        ep_copy(d).wait_recv()
        share_out(d)

    every(1, arrived)

    def pass_on(d):
        for h in range(1, n_y):
            y_copy(d, h).wait_recv()
            forward_copy(d, h).start()

    every(0, pass_on)

    def close(d):
        core_copy(d).wait()
        for h in range(1, n_y):
            y_copy(d, h).wait_send()
            forward_copy(d, h).wait()

    every(0, close)

    def close_far(d):
        ep_copy(d).wait_send()
        ends_copy(d).wait()

    every(1, close_far)
    own_ends.wait()


def return_kernel(
    part_ref,
    proj_ref,
    home_ref,
    mixer_ref,
    near_ref,
    stage_ref,
    far_ref,
    final_ref,
    mnear_ref,
    mstage_ref,
    mfar_ref,
    own_sem,
    ns,
    nr,
    ys,
    yr,
    es,
    er,
    mns,
    mnr,
    mys,
    myr,
):
    n_ep, n_tp, n_y, e, t, y, core = place_of()
    share = part_ref.shape[2] // n_tp
    rows = proj_ref.shape[0] // n_tp
    other = 2 * y + 1 - core

    def columns(index):
        return pl.ds(pl.multiple_of(index * share, share), share)

    def row_block(index):
        return pl.ds(pl.multiple_of(index * rows, rows), rows)

    def peer_y(h):
        return lax.rem(y + h, n_y)

    def near_copy(s, h):
        src = part_ref.at[s, :, columns(2 * peer_y(h) + 1 - core)]
        return remote(src, near_ref.at[s, h], ns.at[s, h], nr.at[s, h], e, other)

    def y_copy(s, h):
        return remote(
            stage_ref.at[s, h], far_ref.at[s, h], ys.at[s, h], yr.at[s, h], e, 2 * peer_y(h) + core
        )

    def home_of(d):
        return lax.rem(e + d, n_ep)

    def home_copy(d):
        peer = home_of(d)
        return remote(final_ref.at[peer], home_ref.at[e], es.at[d], er.at[d], peer, t)

    def mnear_copy(h):
        src = proj_ref.at[row_block(2 * peer_y(h) + 1 - core), :]
        return remote(src, mnear_ref.at[h], mns.at[h], mnr.at[h], e, other)

    def my_copy(h):
        return remote(
            mstage_ref.at[h], mfar_ref.at[h], mys.at[h], myr.at[h], e, 2 * peer_y(h) + core
        )

    def every(first, body):
        def run(d, carry):
            body(d)
            return carry

        lax.fori_loop(first, n_ep, run, 0)

    meet()

    def start_near(d):
        for h in range(n_y):
            near_copy(home_of(d), h).start()

    every(1, start_near)
    start_near(0)
    for h in range(n_y):
        mnear_copy(h).start()

    def wide(x):
        return x.astype(jnp.float32)

    def pair_sum(s, h):
        return wide(part_ref[s, :, columns(2 * peer_y(h) + core)]) + wide(near_ref[s, h])

    def add_near(s):
        for h in range(1, n_y):
            near_copy(s, h).wait_recv()
            stage_ref[s, h] = bf(pair_sum(s, h))
            y_copy(s, h).start()

    every(1, lambda d: add_near(home_of(d)))
    add_near(e)

    def mixer_sum(h):
        return wide(proj_ref[row_block(2 * peer_y(h) + core), :]) + wide(mnear_ref[h])

    for h in range(1, n_y):
        mnear_copy(h).wait_recv()
        mstage_ref[h] = bf(mixer_sum(h))
        my_copy(h).start()

    def add_far(s):
        near_copy(s, 0).wait_recv()
        total = pair_sum(s, 0)
        for h in range(1, n_y):
            y_copy(s, h).wait_recv()
            total = total + wide(far_ref[s, h])
        return bf(total)

    def go_home(d):
        s = home_of(d)
        final_ref[s] = add_far(s)
        home_copy(d).start()

    every(1, go_home)
    home_ref[e] = add_far(e)

    mnear_copy(0).wait_recv()
    total = mixer_sum(0)
    for h in range(1, n_y):
        my_copy(h).wait_recv()
        total = total + wide(mfar_ref[h])
    mixer_ref[...] = bf(total)

    def close(s):
        for h in range(n_y):
            near_copy(s, h).wait_send()
        for h in range(1, n_y):
            y_copy(s, h).wait_send()

    every(0, close)
    for h in range(n_y):
        mnear_copy(h).wait_send()
    for h in range(1, n_y):
        my_copy(h).wait_send()
    every(1, lambda d: home_copy(d).wait())


def exchange_out(own_columns, ends):
    n_ep, n_tp = lax.axis_size("ep"), lax.axis_size("tp")
    n_y = n_tp // 2
    capacity, share = own_columns.shape[1:]
    one, many = pltpu.SemaphoreType.DMA((n_ep,)), pltpu.SemaphoreType.DMA((n_y, n_ep))
    return pl.pallas_call(
        dispatch_kernel,
        out_shape=(
            jax.ShapeDtypeStruct((n_ep, capacity, n_tp * share), jnp.bfloat16),
            jax.ShapeDtypeStruct((n_ep, *ends.shape), jnp.bfloat16),
        ),
        in_specs=[pl.BlockSpec(memory_space=pltpu.VMEM)] * 2,
        out_specs=[pl.BlockSpec(memory_space=pltpu.VMEM)] * 2,
        scratch_shapes=[pltpu.SemaphoreType.DMA((2,))] + [one] * 6 + [many] * 4,
        compiler_params=pltpu.CompilerParams(collective_id=0, has_side_effects=True),
    )(own_columns, ends)


def exchange_back(partial_rows, projected):
    n_ep, n_tp = lax.axis_size("ep"), lax.axis_size("tp")
    n_y = n_tp // 2
    capacity, model = partial_rows.shape[1:]
    share, rows = model // n_tp, projected.shape[0] // n_tp
    many, few = pltpu.SemaphoreType.DMA((n_ep, n_y)), pltpu.SemaphoreType.DMA((n_y,))
    one = pltpu.SemaphoreType.DMA((n_ep,))

    def held(*shape):
        return pltpu.VMEM(shape, jnp.bfloat16)

    return pl.pallas_call(
        return_kernel,
        out_shape=(
            jax.ShapeDtypeStruct((n_ep, capacity, share), jnp.bfloat16),
            jax.ShapeDtypeStruct((rows, model), jnp.bfloat16),
        ),
        in_specs=[pl.BlockSpec(memory_space=pltpu.VMEM)] * 2,
        out_specs=[pl.BlockSpec(memory_space=pltpu.VMEM)] * 2,
        scratch_shapes=[held(n_ep, n_y, capacity, share)] * 3
        + [held(n_ep, capacity, share)]
        + [held(n_y, rows, model)] * 3
        + [pltpu.SemaphoreType.DMA((1,))]
        + [many] * 4
        + [one] * 2
        + [few] * 4,
        compiler_params=pltpu.CompilerParams(collective_id=1, has_side_effects=True),
    )(partial_rows, projected)


def mixer_scan(
    receptance,
    key_matrix,
    value_matrix,
    decay_data_term,
    correction_rate_data,
    output_gate_input,
    decay_channel_offset,
    correction_rate_offset,
    extra_head_log_decay,
    head_norm_gain,
):
    positions, own_width = receptance.shape
    pairs = -(-own_width // PAIR)
    width = pairs * PAIR

    def filled(x, columns=width):
        return x if x.shape[-1] == columns else jnp.pad(x, ((0, 0), (0, columns - x.shape[-1])))

    blocks = positions // HEAD_DIM
    group = 4 if blocks % 4 == 0 else 1
    local, reach, ends = pl.pallas_call(
        functools.partial(scan_kernel, group),
        out_shape=(
            jax.ShapeDtypeStruct((positions, width), jnp.float32),
            jax.ShapeDtypeStruct((positions, width), jnp.bfloat16),
            jax.ShapeDtypeStruct((pairs * 2 * HEAD_DIM, PAIR), jnp.bfloat16),
        ),
        scratch_shapes=[pltpu.VMEM((pairs, 2 * PAIR, PAIR), jnp.float32)],
        cost_estimate=pl.CostEstimate(
            flops=60000 * positions * width, bytes_accessed=16 * positions * width, transcendentals=0
        ),
    )(
        filled(receptance),
        filled(key_matrix),
        filled(value_matrix),
        filled(decay_data_term),
        filled(correction_rate_data),
        filled(decay_channel_offset[None]),
        filled(correction_rate_offset[None]),
        filled(extra_head_log_decay, 2 * pairs),
    )
    return local, reach, ends, filled(output_gate_input), filled(head_norm_gain[None])


def mixer_finish(everyone, local, reach, gate_input, gain, mixer_output_weight):
    positions, width = local.shape
    own_width = mixer_output_weight.shape[0]
    mixed_hidden = pl.pallas_call(
        functools.partial(join_kernel, "ep"),
        out_shape=jax.ShapeDtypeStruct((positions, width), jnp.bfloat16),
        cost_estimate=pl.CostEstimate(
            flops=6000 * positions * width, bytes_accessed=16 * positions * width, transcendentals=0
        ),
    )(everyone, local, reach, gate_input, gain)
    mixed_hidden = mixed_hidden[:, :own_width]
    return jnp.dot(mixed_hidden, mixer_output_weight, preferred_element_type=jnp.float32).astype(
        jnp.bfloat16
    )


def expert_route(
    expert_layer_input,
    feedforward_norm_gain,
    group_router_weight,
    expert_router_weight,
    routes,
):
    token_rows = expert_layer_input.shape[0]
    route_count = routes.shape[1]
    ep_count = lax.axis_size("ep")
    expert_total = expert_router_weight.shape[1]
    per_group = expert_total // GROUPS
    capacity = 4 * token_rows // ep_count
    widened = expert_layer_input.astype(jnp.float32)
    normed_input = (
        widened
        * lax.rsqrt(jnp.mean(widened * widened, axis=-1, keepdims=True) + norm_eps)
        * feedforward_norm_gain
    ).astype(jnp.bfloat16)
    group_logit = jnp.dot(normed_input, group_router_weight, preferred_element_type=jnp.float32)
    group_exp = jnp.exp(group_logit)
    group_prob = group_exp / jnp.sum(group_exp, axis=-1, keepdims=True)
    expert_logit = jnp.dot(normed_input, expert_router_weight, preferred_element_type=jnp.float32)
    expert_range = jnp.arange(expert_total, dtype=jnp.int32)
    matched = routes[:, :, None] == expert_range[None, None, :]
    chosen_logit = jnp.sum(jnp.where(matched, expert_logit[:, None, :], 0.0), axis=-1)
    group_match = (routes // per_group)[:, :, None] == jnp.arange(GROUPS, dtype=jnp.int32)[
        None, None, :
    ]
    chosen_group = jnp.sum(jnp.where(group_match, group_prob[:, None, :], 0.0), axis=-1)
    route_weight = chosen_group * jax.nn.sigmoid(chosen_logit - chosen_logit[:, ::-1])
    flat_match = matched.reshape(token_rows * route_count, expert_total).astype(jnp.int32)
    before = jnp.cumsum(flat_match, axis=0) - flat_match
    placed = jnp.sum(before * flat_match, axis=1)
    slot_ids = routes.reshape(-1) * capacity + placed
    slot_range = jnp.arange(expert_total * capacity, dtype=jnp.int32)
    struck = (slot_range[:, None] == slot_ids[None, :]).reshape(
        expert_total * capacity, token_rows, route_count
    )
    dispatch_matrix = jnp.any(struck, axis=-1).astype(jnp.bfloat16)
    combine_matrix = jnp.sum(jnp.where(struck, route_weight[None, :, :], 0.0), axis=-1)
    outgoing = jnp.dot(dispatch_matrix, normed_input, preferred_element_type=jnp.float32).astype(
        jnp.bfloat16
    )
    outgoing = outgoing.reshape(ep_count, capacity, outgoing.shape[1])
    width_share = outgoing.shape[2] // lax.axis_size("tp")
    own_columns = lax.dynamic_slice_in_dim(
        outgoing, lax.axis_index("tp") * width_share, width_share, 2
    )
    return own_columns, combine_matrix


def expert_rows(piece, expert_gate_weight, expert_up_weight, expert_down_weight):
    rows = piece.reshape(-1, piece.shape[2])
    gate_val = jnp.dot(rows, expert_gate_weight[0], preferred_element_type=jnp.float32)
    up_val = jnp.dot(rows, expert_up_weight[0], preferred_element_type=jnp.float32)
    expert_hidden = (jax.nn.silu(gate_val) * up_val).astype(jnp.bfloat16)
    result = jnp.dot(expert_hidden, expert_down_weight[0], preferred_element_type=jnp.float32)
    return result.astype(jnp.bfloat16).reshape(piece.shape)


def expert_combine(homebound, combine_matrix):
    homebound = homebound.reshape(-1, homebound.shape[2]).astype(jnp.float32)
    combined = lax.dot_general(
        combine_matrix, homebound, (((0,), (0,)), ((), ())), precision=highest
    )
    return combined.astype(jnp.bfloat16)


def local(
    receptance,
    key_matrix,
    value_matrix,
    decay_data_term,
    correction_rate_data,
    output_gate_input,
    decay_channel_offset,
    correction_rate_offset,
    extra_head_log_decay,
    head_norm_gain,
    mixer_output_weight,
    expert_layer_input,
    feedforward_norm_gain,
    group_router_weight,
    expert_router_weight,
    routes,
    expert_gate_weight,
    expert_up_weight,
    expert_down_weight,
):
    local_read, reach, ends, gate_input, gain = mixer_scan(
        receptance,
        key_matrix,
        value_matrix,
        decay_data_term,
        correction_rate_data,
        output_gate_input,
        decay_channel_offset,
        correction_rate_offset,
        extra_head_log_decay,
        head_norm_gain,
    )
    own_columns, combine_matrix = expert_route(
        expert_layer_input,
        feedforward_norm_gain,
        group_router_weight,
        expert_router_weight,
        routes,
    )
    piece, everyone = exchange_out(own_columns, ends)
    projected = mixer_finish(everyone, local_read, reach, gate_input, gain, mixer_output_weight)
    partial_rows = expert_rows(piece, expert_gate_weight, expert_up_weight, expert_down_weight)
    homebound, token_mixer_output = exchange_back(partial_rows, projected)
    return (token_mixer_output, expert_combine(homebound, combine_matrix))


def solution(mesh):
    in_specs = (
        P("ep", "tp"),
        P("ep", "tp"),
        P("ep", "tp"),
        P("ep", "tp"),
        P("ep", "tp"),
        P("ep", "tp"),
        P("tp"),
        P("tp"),
        P("ep", "tp"),
        P("tp"),
        P("tp", None),
        P("ep", None),
        P(),
        P(),
        P(),
        P("ep", None),
        P("ep", None, "tp"),
        P("ep", None, "tp"),
        P("ep", "tp", None),
    )
    out_specs = (P(("ep", "tp"), None), P("ep", "tp"))
    return jax.shard_map(local, mesh=mesh, in_specs=in_specs, out_specs=out_specs, check_vma=False)
```

```python
import functools
import math

import jax
import jax.numpy as jnp
from jax import lax
from jax.experimental import pallas as pl
from jax.experimental.pallas import tpu as pltpu
from jax.sharding import PartitionSpec as P

HEAD_DIM = 64
PAIR = 2 * HEAD_DIM
HALF_EXP = math.exp(-0.5)
GROUPS = 4


key_eps = 1e-06
group_eps = 0.00064
norm_eps = 1e-06
highest = lax.Precision.HIGHEST


def bf(x):
    return x.astype(jnp.bfloat16)


def mm(x, y):
    return lax.dot_general(x, y, (((1,), (0,)), ((), ())), preferred_element_type=jnp.float32)


def mm_nt(x, y):
    return lax.dot_general(x, y, (((1,), (1,)), ((), ())), preferred_element_type=jnp.float32)


def mm_tn(x, y):
    return lax.dot_general(x, y, (((0,), (0,)), ((), ())), preferred_element_type=jnp.float32)


def halves(x):
    high = bf(x)
    return high, bf(x - high.astype(jnp.float32))


def sum_right(x, ones):
    high, low = halves(x)
    return mm(high, ones) + mm(low, ones)


def logistic(x):
    return 1.0 / (1.0 + jnp.exp(-x))


def flag(cond):
    return jnp.where(cond, 1.0, 0.0)


def iota(shape, dim):
    return lax.broadcasted_iota(jnp.int32, shape, dim)


def pair_blocks():
    return flag((iota((PAIR, PAIR), 0) < HEAD_DIM) == (iota((PAIR, PAIR), 1) < HEAD_DIM))


def scan_kernel(
    group,
    r_ref,
    k_ref,
    v_ref,
    d_ref,
    a_ref,
    d_off_ref,
    a_off_ref,
    extra_ref,
    out_ref,
    reach_ref,
    ends_ref,
    chain_ref,
):
    positions, width = r_ref.shape
    pairs = width // PAIR
    C = HEAD_DIM
    rows_per = group * C
    own_block = pair_blocks()
    own_bf = bf(own_block)
    row, col = iota((C, PAIR), 0), iota((C, PAIR), 1) & (HEAD_DIM - 1)
    strict, upto = row > col, row >= col
    eye = flag(row == col)
    first = iota((1, PAIR), 1) < HEAD_DIM
    tri = bf(flag(iota((C, C), 0) >= iota((C, C), 1)))
    level_masks = []
    for s in range(6):
        inside = (
            ((row >> (s + 1)) == (col >> (s + 1)))
            & (((row >> s) & 1) == 1)
            & (((col >> s) & 1) == 0)
        )
        level_masks.append(bf(flag(inside)))

    def spread(x):
        return jnp.concatenate([x, x], axis=0) * own_bf

    square = (iota((PAIR, PAIR), 0) == iota((PAIR, PAIR), 1)).astype(jnp.float32)
    for p in range(pairs):
        chain_ref[p, :PAIR] = jnp.zeros((PAIR, PAIR), jnp.float32)
        chain_ref[p, PAIR:] = square

    def step(g, carry):
        base = pl.multiple_of(g * rows_per, rows_per)
        rows = pl.ds(base, rows_per)
        items = []
        for p in range(pairs):
            lanes = slice(p * PAIR, (p + 1) * PAIR)
            k = k_ref[rows, lanes].astype(jnp.float32)
            u = k * lax.rsqrt(sum_right(k * k, own_bf) + key_eps)
            rem = u * logistic(a_ref[rows, lanes].astype(jnp.float32) + a_off_ref[:, lanes])
            e = extra_ref[rows, :]
            extra = jnp.where(first, e[:, 2 * p : 2 * p + 1], e[:, 2 * p + 1 : 2 * p + 2])
            lg = extra - HALF_EXP * logistic(
                d_ref[rows, lanes].astype(jnp.float32) + d_off_ref[:, lanes]
            )
            r = r_ref[rows, lanes].astype(jnp.float32)
            v = v_ref[rows, lanes]
            for c in range(group):
                cut = slice(c * C, (c + 1) * C)
                items.append((p, c, k[cut], u[cut], rem[cut], lg[cut], r[cut], v[cut]))
        stage = []
        for p, c, k, u, rem, lg, r, v in items:
            high, low = halves(lg)
            rest = bf(lg - high.astype(jnp.float32) - low.astype(jnp.float32))
            cumul = mm(tri, high) + mm(tri, low) + mm(tri, rest)
            stage.append(cumul)
        work = []
        for (p, c, k, u, rem, lg, r, v), cumul in zip(items, stage):
            mid = 0.5 * cumul[C - 1 : C]
            up_now, down = jnp.exp(cumul - mid), jnp.exp(mid - cumul)
            up_before = jnp.exp(cumul - lg - mid)
            half = jnp.exp(mid)
            cq, cu, dk, dr = r * up_now, u * up_before, k * down, rem * down
            left = bf(jnp.concatenate([cu, cq], axis=0))
            pair_r = mm_nt(left, spread(bf(dr)))
            pair_k = mm_nt(left, spread(bf(dk)))
            work.append((cq * half, bf(cu * half), bf(dk * half), bf(dr * half), half * half, pair_r, pair_k))
        solve = []
        for (p, c, k, u, rem, lg, r, v), (qe, ue, kt, rt, ed, pair_r, pair_k) in zip(items, work):
            rp = bf(jnp.where(strict, pair_r[:C], 0.0))
            rr = bf(jnp.where(upto, pair_r[C:], 0.0))
            kp = jnp.where(strict, pair_k[:C], 0.0)
            rk = jnp.where(upto, pair_k[C:], 0.0)
            kv = mm(bf(jnp.concatenate([kp, rk], axis=0)), spread(v))
            inv = eye - (rp * level_masks[0]).astype(jnp.float32)
            solve.append([rp, rr, kv, inv])
        for s in range(1, 6):
            mids = [bf(mm(bf(inv), spread(rp * level_masks[s]))) for rp, rr, kv, inv in solve]
            for item, y in zip(solve, mids):
                item[3] = item[3] - mm(y, spread(bf(item[3])))
        wvs = []
        for (rp, rr, kv, inv), w in zip(solve, work):
            wide = jnp.concatenate([spread(w[1]), spread(bf(kv[:C]))], axis=1)
            wvs.append(bf(mm(bf(inv), wide)))
        tails = []
        for (rp, rr, kv, inv), (qe, ue, kt, rt, ed, _, _), wv, item in zip(solve, work, wvs, items):
            wide = jnp.concatenate([spread(wv[:, :PAIR]), spread(wv[:, PAIR:])], axis=1)
            rw = mm(rr, wide)
            read = bf(qe - rw[:, :PAIR])
            local = kv[C:] - rw[:, PAIR:]
            v = item[7]
            x = jnp.concatenate(
                [jnp.concatenate([v, jnp.zeros_like(v)], axis=1),
                 jnp.concatenate([-wv[:, PAIR:], -wv[:, :PAIR]], axis=1)], axis=0)
            nb = mm_tn(x, jnp.concatenate([kt, rt], axis=0))
            tails.append((read, local, nb[:PAIR] * own_block, bf(nb[PAIR:] * own_block), ed))
        z = [chain_ref[p] for p in range(pairs)]
        for c in range(group):
            for p in range(pairs):
                read, local, add, neg, ed = tails[p * group + c]
                zb = bf(z[p])
                qz = mm_nt(read, zb)
                at = pl.ds(pl.multiple_of(base + c * C, C), C)
                lanes = slice(p * PAIR, (p + 1) * PAIR)
                out_ref[at, lanes] = local + qz[:, :PAIR]
                reach_ref[at, lanes] = bf(qz[:, PAIR:])
                moved = z[p] * ed + mm(zb, neg)
                z[p] = jnp.concatenate([moved[:PAIR] + add, moved[PAIR:]], axis=0)
        for p in range(pairs):
            chain_ref[p] = z[p]
        return carry

    lax.fori_loop(0, positions // rows_per, step, 0)
    for p in range(pairs):
        s, m = chain_ref[p, :PAIR], chain_ref[p, PAIR:]
        ends_ref[p * 2 * C : p * 2 * C + C] = bf(s[:C] + s[C:])
        ends_ref[p * 2 * C + C : (p + 1) * 2 * C] = bf(m[:C] + m[C:])


def join_kernel(axis, all_ref, out_ref, reach_ref, gate_ref, gain_ref, mixed_ref):
    devices, place = lax.axis_size(axis), lax.axis_index(axis)
    width = out_ref.shape[1]
    pairs = width // PAIR
    C = HEAD_DIM
    own_block = pair_blocks()
    own_bf = bf(own_block)
    mean_bf = bf(own_block * (1.0 / HEAD_DIM))
    states = [jnp.zeros((C, PAIR), jnp.float32) for _ in range(pairs)]

    def hop(j, states):
        new = []
        for p in range(pairs):
            s = all_ref[j, p * 2 * C : p * 2 * C + C].astype(jnp.float32)
            m = all_ref[j, p * 2 * C + C : (p + 1) * 2 * C]
            m = jnp.concatenate([m, m], axis=0) * own_bf
            new.append(sum_right(states[p], m) + s)
        return tuple(new)

    states = lax.fori_loop(0, place, hop, tuple(states))
    for p in range(pairs):
        lanes = slice(p * PAIR, (p + 1) * PAIR)
        s = bf(states[p])
        s = jnp.concatenate([s, s], axis=0) * own_bf
        head = out_ref[:, lanes] + mm_nt(reach_ref[:, lanes], s)
        centred = head - sum_right(head, mean_bf)
        spread = sum_right(centred * centred, mean_bf)
        normed = centred * lax.rsqrt(spread + group_eps)
        gate = logistic(gate_ref[:, lanes].astype(jnp.float32))
        mixed_ref[:, lanes] = bf(normed * gain_ref[:, lanes] * gate)


def place_of():
    n_ep, n_tp = lax.axis_size("ep"), lax.axis_size("tp")
    e, t = lax.axis_index("ep"), lax.axis_index("tp")
    core = lax.rem(t, 2)
    return n_ep, n_tp, n_tp // 2, e, t, lax.div(t, 2), core


def remote(src, dst, send, recv, e, t):
    return pltpu.make_async_remote_copy(
        src_ref=src,
        dst_ref=dst,
        send_sem=send,
        recv_sem=recv,
        device_id=(e, t),
        device_id_type=pl.DeviceIdType.MESH,
    )


def meet():
    n_ep, n_tp, n_y, e, t, y, core = place_of()
    barrier = pltpu.get_barrier_semaphore()

    def greet(pe, pt):
        pl.semaphore_signal(
            barrier, inc=1, device_id=(pe, pt), device_id_type=pl.DeviceIdType.MESH
        )

    for d in range(1, n_ep):
        greet(lax.rem(e + d, n_ep), t)
    greet(e, 2 * y + 1 - core)
    for d in range(1, n_y):
        greet(e, 2 * lax.rem(y + d, n_y) + core)
    pl.semaphore_wait(barrier, n_ep - 1 + n_y)


def dispatch_kernel(
    group,
    r_ref,
    k_ref,
    v_ref,
    d_ref,
    a_ref,
    d_off_ref,
    a_off_ref,
    extra_ref,
    cols_ref,
    out_ref,
    reach_ref,
    piece_ref,
    every_ref,
    chain_ref,
    ends_ref,
    own_sem,
    es,
    er,
    gs,
    gr,
    cs,
    cr,
    ys,
    yr,
    fs,
    fr,
):
    n_ep, n_tp, n_y, e, t, y, core = place_of()
    share = cols_ref.shape[2]
    other = 2 * y + 1 - core

    def columns(index):
        return pl.ds(pl.multiple_of(index * share, share), share)

    def block(source, index):
        return piece_ref.at[source, :, columns(index)]

    meet()
    own = pltpu.make_async_copy(cols_ref.at[e], block(e, t), own_sem.at[0])
    own_ends = pltpu.make_async_copy(ends_ref, every_ref.at[e], own_sem.at[1])
    own.start()

    def ep_copy(d):
        peer = lax.rem(e + d, n_ep)
        return remote(cols_ref.at[peer], block(e, t), es.at[d], er.at[d], peer, t)

    def ends_copy(d):
        peer = lax.rem(e + d, n_ep)
        return remote(ends_ref, every_ref.at[e], gs.at[d], gr.at[d], peer, t)

    def source(d):
        return lax.rem(e - d + n_ep, n_ep)

    def core_copy(d):
        return remote(block(source(d), t), block(source(d), t), cs.at[d], cr.at[d], e, other)

    def y_copy(d, h):
        peer = 2 * lax.rem(y + h, n_y) + core
        return remote(block(source(d), t), block(source(d), t), ys.at[h, d], yr.at[h, d], e, peer)

    def forward_copy(d, h):
        index = 2 * lax.rem(y - h + n_y, n_y) + core
        return remote(
            block(source(d), index), block(source(d), index), fs.at[h, d], fr.at[h, d], e, other
        )

    def every(first, body):
        def run(d, carry):
            body(d)
            return carry

        lax.fori_loop(first, n_ep, run, 0)

    every(1, lambda d: ep_copy(d).start())

    def share_out(d):
        core_copy(d).start()
        for h in range(1, n_y):
            y_copy(d, h).start()

    own.wait()
    share_out(0)
    scan_kernel(
        group,
        r_ref,
        k_ref,
        v_ref,
        d_ref,
        a_ref,
        d_off_ref,
        a_off_ref,
        extra_ref,
        out_ref,
        reach_ref,
        ends_ref,
        chain_ref,
    )

    def arrived(d):
        ep_copy(d).wait_recv()
        share_out(d)

    every(1, arrived)
    every(1, lambda d: ends_copy(d).start())
    own_ends.start()

    def pass_on(d):
        for h in range(1, n_y):
            y_copy(d, h).wait_recv()
            forward_copy(d, h).start()

    every(0, pass_on)

    def close(d):
        core_copy(d).wait()
        for h in range(1, n_y):
            y_copy(d, h).wait_send()
            forward_copy(d, h).wait()

    every(0, close)

    def close_far(d):
        ep_copy(d).wait_send()
        ends_copy(d).wait()

    every(1, close_far)
    own_ends.wait()


def return_kernel(
    piece_ref,
    proj_ref,
    gate_hbm,
    up_hbm,
    down_hbm,
    home_ref,
    mixer_ref,
    gate_ref,
    up_ref,
    down_ref,
    rows_ref,
    hidden_ref,
    part_ref,
    near_ref,
    stage_ref,
    far_ref,
    final_ref,
    mnear_ref,
    mstage_ref,
    mfar_ref,
    gate_sem,
    up_sem,
    down_sem,
    ns,
    nr,
    ys,
    yr,
    es,
    er,
    mns,
    mnr,
    mys,
    myr,
):
    n_ep, n_tp, n_y, e, t, y, core = place_of()
    capacity, model = part_ref.shape[1:]
    units = gate_ref.shape[1]
    share = model // n_tp
    rows = proj_ref.shape[0] // (2 * n_tp)
    other = 2 * y + 1 - core
    half = n_ep // 2
    wide_units, wide_model = min(256, units), min(512, model)

    def gate_copy(i):
        at = pl.ds(pl.multiple_of(i * wide_units, wide_units), wide_units)
        return (
            pltpu.make_async_copy(gate_hbm.at[0, :, at], gate_ref.at[:, at], gate_sem.at[i]),
            pltpu.make_async_copy(up_hbm.at[0, :, at], up_ref.at[:, at], up_sem.at[i]),
        )

    def down_copy(i):
        at = pl.ds(pl.multiple_of(i * wide_model, wide_model), wide_model)
        return pltpu.make_async_copy(down_hbm.at[0, :, at], down_ref.at[:, at], down_sem.at[i])

    for i in range(units // wide_units):
        for copy in gate_copy(i):
            copy.start()
    for i in range(model // wide_model):
        down_copy(i).start()

    def columns(index):
        return pl.ds(pl.multiple_of(index * share, share), share)

    def row_block(index, q):
        return pl.ds(pl.multiple_of((2 * index + q) * rows, rows), rows)

    def peer_y(h):
        return lax.rem(y + h, n_y)

    def near_copy(s, h):
        src = part_ref.at[s, :, columns(2 * peer_y(h) + 1 - core)]
        return remote(src, near_ref.at[s, h], ns.at[s, h], nr.at[s, h], e, other)

    def y_copy(s, h):
        return remote(
            stage_ref.at[s, h], far_ref.at[s, h], ys.at[s, h], yr.at[s, h], e, 2 * peer_y(h) + core
        )

    def offset(k):
        m = lax.div(k + 1, 2)
        return lax.rem(half + m * (2 * lax.rem(k, 2) - 1) + n_ep, n_ep)

    def home_of(k):
        return lax.rem(e + offset(k), n_ep)

    def home_copy(k):
        peer, d = home_of(k), offset(k)
        return remote(final_ref.at[peer], home_ref.at[e], es.at[d], er.at[d], peer, t)

    def mnear_copy(q, h):
        src = proj_ref.at[row_block(2 * peer_y(h) + 1 - core, q), :]
        return remote(src, mnear_ref.at[q, h], mns.at[q, h], mnr.at[q, h], e, other)

    def my_copy(q, h):
        target = 2 * peer_y(h) + core
        return remote(
            mstage_ref.at[q, h], mfar_ref.at[q, h], mys.at[q, h], myr.at[q, h], e, target
        )

    def span(first, last, body):
        def run(d, carry):
            body(d)
            return carry

        lax.fori_loop(first, last, run, 0)

    def wide(x):
        return x.astype(jnp.float32)

    def mixer_sum(q, h):
        return wide(proj_ref[row_block(2 * peer_y(h) + core, q), :]) + wide(mnear_ref[q, h])

    def mixer_share(q):
        for h in range(1, n_y):
            mnear_copy(q, h).wait_recv()
            mstage_ref[q, h] = bf(mixer_sum(q, h))
            my_copy(q, h).start()

    def mixer_end(q):
        mnear_copy(q, 0).wait_recv()
        total = mixer_sum(q, 0)
        for h in range(1, n_y):
            my_copy(q, h).wait_recv()
            total = total + wide(mfar_ref[q, h])
        mixer_ref[q * rows : (q + 1) * rows] = bf(total)

    def widen(b):
        def take(k):
            at = pl.ds(pl.multiple_of((k - b * half) * capacity, capacity), capacity)
            rows_ref[at, :] = piece_ref[home_of(k)]

        span(b * half, (b + 1) * half, take)

        def unit_tile(i):
            if b == 0:
                for copy in gate_copy(i):
                    copy.wait()
            at = pl.ds(pl.multiple_of(i * wide_units, wide_units), wide_units)
            x = rows_ref[...]
            gate_val = mm(x, gate_ref[:, at])
            hidden_ref[:, at] = bf(gate_val * logistic(gate_val) * mm(x, up_ref[:, at]))

        span(0, units // wide_units, unit_tile)

    def narrow(b):
        def model_tile(i):
            if b == 0:
                down_copy(i).wait()
            at = pl.ds(pl.multiple_of(i * wide_model, wide_model), wide_model)
            result = bf(mm(hidden_ref[...], down_ref[:, at]))
            for j in range(half):
                part_ref[home_of(b * half + j), :, at] = result[j * capacity : (j + 1) * capacity]

        span(0, model // wide_model, model_tile)

    def start_near(k):
        for h in range(n_y):
            near_copy(home_of(k), h).start()

    def pair_sum(s, h):
        return wide(part_ref[s, :, columns(2 * peer_y(h) + core)]) + wide(near_ref[s, h])

    def add_near(k):
        s = home_of(k)
        for h in range(1, n_y):
            near_copy(s, h).wait_recv()
            stage_ref[s, h] = bf(pair_sum(s, h))
            y_copy(s, h).start()

    def add_far(s):
        near_copy(s, 0).wait_recv()
        total = pair_sum(s, 0)
        for h in range(1, n_y):
            y_copy(s, h).wait_recv()
            total = total + wide(far_ref[s, h])
        return bf(total)

    def go_home(k):
        s = home_of(k)
        final_ref[s] = add_far(s)
        home_copy(k).start()

    meet()
    for q in range(2):
        for h in range(n_y):
            mnear_copy(q, h).start()
    mixer_share(0)
    widen(0)
    narrow(0)
    span(0, half, start_near)
    widen(1)
    span(0, half, add_near)
    narrow(1)
    span(half, n_ep, start_near)
    span(half, n_ep, add_near)
    mixer_share(1)
    span(0, half, go_home)
    mixer_end(0)
    span(half, n_ep - 1, go_home)
    home_ref[e] = add_far(e)
    mixer_end(1)

    def close(s):
        for h in range(n_y):
            near_copy(s, h).wait_send()
        for h in range(1, n_y):
            y_copy(s, h).wait_send()

    span(0, n_ep, close)
    for q in range(2):
        for h in range(n_y):
            mnear_copy(q, h).wait_send()
        for h in range(1, n_y):
            my_copy(q, h).wait_send()
    span(0, n_ep - 1, lambda k: home_copy(k).wait())


def experts_and_back(piece, projected, gate_weight, up_weight, down_weight):
    n_ep, n_tp = lax.axis_size("ep"), lax.axis_size("tp")
    n_y = n_tp // 2
    capacity, model = piece.shape[1:]
    units = gate_weight.shape[2]
    share, rows = model // n_tp, projected.shape[0] // n_tp
    many, few = pltpu.SemaphoreType.DMA((n_ep, n_y)), pltpu.SemaphoreType.DMA((2, n_y))
    one = pltpu.SemaphoreType.DMA((n_ep,))

    def held(*shape):
        return pltpu.VMEM(shape, jnp.bfloat16)

    in_vmem = pl.BlockSpec(memory_space=pltpu.VMEM)
    return pl.pallas_call(
        return_kernel,
        out_shape=(
            jax.ShapeDtypeStruct((n_ep, capacity, share), jnp.bfloat16),
            jax.ShapeDtypeStruct((rows, model), jnp.bfloat16),
        ),
        in_specs=[in_vmem] * 2 + [pl.BlockSpec(memory_space=pl.ANY)] * 3,
        out_specs=[in_vmem] * 2,
        scratch_shapes=[
            held(model, units),
            held(model, units),
            held(units, model),
            held(n_ep // 2 * capacity, model),
            held(n_ep // 2 * capacity, units),
            held(n_ep, capacity, model),
        ]
        + [held(n_ep, n_y, capacity, share)] * 3
        + [held(n_ep, capacity, share)]
        + [held(2, n_y, rows // 2, model)] * 3
        + [pltpu.SemaphoreType.DMA((max(1, units // 256),))] * 2
        + [pltpu.SemaphoreType.DMA((max(1, model // 512),))]
        + [many] * 4
        + [one] * 2
        + [few] * 4,
        compiler_params=pltpu.CompilerParams(collective_id=1, has_side_effects=True),
    )(piece, projected, gate_weight, up_weight, down_weight)


def scan_and_dispatch(
    own_columns,
    receptance,
    key_matrix,
    value_matrix,
    decay_data_term,
    correction_rate_data,
    output_gate_input,
    decay_channel_offset,
    correction_rate_offset,
    extra_head_log_decay,
    head_norm_gain,
):
    positions, own_width = receptance.shape
    pairs = -(-own_width // PAIR)
    width = pairs * PAIR

    def filled(x, columns=width):
        return x if x.shape[-1] == columns else jnp.pad(x, ((0, 0), (0, columns - x.shape[-1])))

    blocks = positions // HEAD_DIM
    group = 4 if blocks % 4 == 0 else 1
    n_ep, n_tp = lax.axis_size("ep"), lax.axis_size("tp")
    n_y = n_tp // 2
    capacity, share = own_columns.shape[1:]
    ends = (pairs * 2 * HEAD_DIM, PAIR)
    one, many = pltpu.SemaphoreType.DMA((n_ep,)), pltpu.SemaphoreType.DMA((n_y, n_ep))
    local, reach, piece, everyone = pl.pallas_call(
        functools.partial(dispatch_kernel, group),
        out_shape=(
            jax.ShapeDtypeStruct((positions, width), jnp.float32),
            jax.ShapeDtypeStruct((positions, width), jnp.bfloat16),
            jax.ShapeDtypeStruct((n_ep, capacity, n_tp * share), jnp.bfloat16),
            jax.ShapeDtypeStruct((n_ep, *ends), jnp.bfloat16),
        ),
        in_specs=[pl.BlockSpec(memory_space=pltpu.VMEM)] * 9,
        out_specs=[pl.BlockSpec(memory_space=pltpu.VMEM)] * 4,
        scratch_shapes=[
            pltpu.VMEM((pairs, 2 * PAIR, PAIR), jnp.float32),
            pltpu.VMEM(ends, jnp.bfloat16),
            pltpu.SemaphoreType.DMA((2,)),
        ]
        + [one] * 6
        + [many] * 4,
        compiler_params=pltpu.CompilerParams(collective_id=0, has_side_effects=True),
    )(
        filled(receptance),
        filled(key_matrix),
        filled(value_matrix),
        filled(decay_data_term),
        filled(correction_rate_data),
        filled(decay_channel_offset[None]),
        filled(correction_rate_offset[None]),
        filled(extra_head_log_decay, 2 * pairs),
        own_columns,
    )
    gate_input, gain = filled(output_gate_input), filled(head_norm_gain[None])
    return local, reach, piece, everyone, gate_input, gain


def mixer_finish(everyone, local, reach, gate_input, gain, mixer_output_weight):
    positions, width = local.shape
    own_width = mixer_output_weight.shape[0]
    mixed_hidden = pl.pallas_call(
        functools.partial(join_kernel, "ep"),
        out_shape=jax.ShapeDtypeStruct((positions, width), jnp.bfloat16),
        cost_estimate=pl.CostEstimate(
            flops=6000 * positions * width, bytes_accessed=16 * positions * width, transcendentals=0
        ),
    )(everyone, local, reach, gate_input, gain)
    mixed_hidden = mixed_hidden[:, :own_width]
    return jnp.dot(mixed_hidden, mixer_output_weight, preferred_element_type=jnp.float32).astype(
        jnp.bfloat16
    )


def expert_route(
    expert_layer_input,
    feedforward_norm_gain,
    group_router_weight,
    expert_router_weight,
    routes,
):
    token_rows = expert_layer_input.shape[0]
    route_count = routes.shape[1]
    ep_count = lax.axis_size("ep")
    expert_total = expert_router_weight.shape[1]
    per_group = expert_total // GROUPS
    capacity = 4 * token_rows // ep_count
    widened = expert_layer_input.astype(jnp.float32)
    normed_input = (
        widened
        * lax.rsqrt(jnp.mean(widened * widened, axis=-1, keepdims=True) + norm_eps)
        * feedforward_norm_gain
    ).astype(jnp.bfloat16)
    group_logit = jnp.dot(normed_input, group_router_weight, preferred_element_type=jnp.float32)
    group_exp = jnp.exp(group_logit)
    group_prob = group_exp / jnp.sum(group_exp, axis=-1, keepdims=True)
    expert_logit = jnp.dot(normed_input, expert_router_weight, preferred_element_type=jnp.float32)
    expert_range = jnp.arange(expert_total, dtype=jnp.int32)
    matched = routes[:, :, None] == expert_range[None, None, :]
    chosen_logit = jnp.sum(jnp.where(matched, expert_logit[:, None, :], 0.0), axis=-1)
    group_match = (routes // per_group)[:, :, None] == jnp.arange(GROUPS, dtype=jnp.int32)[
        None, None, :
    ]
    chosen_group = jnp.sum(jnp.where(group_match, group_prob[:, None, :], 0.0), axis=-1)
    route_weight = chosen_group * jax.nn.sigmoid(chosen_logit - chosen_logit[:, ::-1])
    flat_match = matched.reshape(token_rows * route_count, expert_total).astype(jnp.int32)
    before = jnp.cumsum(flat_match, axis=0) - flat_match
    placed = jnp.sum(before * flat_match, axis=1)
    slot_ids = routes.reshape(-1) * capacity + placed
    slot_range = jnp.arange(expert_total * capacity, dtype=jnp.int32)
    struck = (slot_range[:, None] == slot_ids[None, :]).reshape(
        expert_total * capacity, token_rows, route_count
    )
    dispatch_matrix = jnp.any(struck, axis=-1).astype(jnp.bfloat16)
    combine_matrix = jnp.sum(jnp.where(struck, route_weight[None, :, :], 0.0), axis=-1)
    outgoing = jnp.dot(dispatch_matrix, normed_input, preferred_element_type=jnp.float32).astype(
        jnp.bfloat16
    )
    outgoing = outgoing.reshape(ep_count, capacity, outgoing.shape[1])
    width_share = outgoing.shape[2] // lax.axis_size("tp")
    own_columns = lax.dynamic_slice_in_dim(
        outgoing, lax.axis_index("tp") * width_share, width_share, 2
    )
    return own_columns, combine_matrix


def expert_combine(homebound, combine_matrix):
    homebound = homebound.reshape(-1, homebound.shape[2]).astype(jnp.float32)
    combined = lax.dot_general(
        combine_matrix, homebound, (((0,), (0,)), ((), ())), precision=highest
    )
    return combined.astype(jnp.bfloat16)


def local(
    receptance,
    key_matrix,
    value_matrix,
    decay_data_term,
    correction_rate_data,
    output_gate_input,
    decay_channel_offset,
    correction_rate_offset,
    extra_head_log_decay,
    head_norm_gain,
    mixer_output_weight,
    expert_layer_input,
    feedforward_norm_gain,
    group_router_weight,
    expert_router_weight,
    routes,
    expert_gate_weight,
    expert_up_weight,
    expert_down_weight,
):
    own_columns, combine_matrix = expert_route(
        expert_layer_input,
        feedforward_norm_gain,
        group_router_weight,
        expert_router_weight,
        routes,
    )
    local_read, reach, piece, everyone, gate_input, gain = scan_and_dispatch(
        own_columns,
        receptance,
        key_matrix,
        value_matrix,
        decay_data_term,
        correction_rate_data,
        output_gate_input,
        decay_channel_offset,
        correction_rate_offset,
        extra_head_log_decay,
        head_norm_gain,
    )
    projected = mixer_finish(everyone, local_read, reach, gate_input, gain, mixer_output_weight)
    homebound, token_mixer_output = experts_and_back(
        piece, projected, expert_gate_weight, expert_up_weight, expert_down_weight
    )
    return (token_mixer_output, expert_combine(homebound, combine_matrix))


def solution(mesh):
    in_specs = (
        P("ep", "tp"),
        P("ep", "tp"),
        P("ep", "tp"),
        P("ep", "tp"),
        P("ep", "tp"),
        P("ep", "tp"),
        P("tp"),
        P("tp"),
        P("ep", "tp"),
        P("tp"),
        P("tp", None),
        P("ep", None),
        P(),
        P(),
        P(),
        P("ep", None),
        P("ep", None, "tp"),
        P("ep", None, "tp"),
        P("ep", "tp", None),
    )
    out_specs = (P(("ep", "tp"), None), P("ep", "tp"))
    return jax.shard_map(local, mesh=mesh, in_specs=in_specs, out_specs=out_specs, check_vma=False)
```

```python
import functools
import math

import jax
import jax.numpy as jnp
from jax import lax
from jax.experimental import pallas as pl
from jax.experimental.pallas import tpu as pltpu
from jax.sharding import PartitionSpec as P

HEAD_DIM = 64
PAIR = 2 * HEAD_DIM
BACK_LIMIT = 44 << 20
HALF_EXP = math.exp(-0.5)
GROUPS = 4


key_eps = 1e-06
group_eps = 0.00064
norm_eps = 1e-06
highest = lax.Precision.HIGHEST


def bf(x):
    return x.astype(jnp.bfloat16)


def mm(x, y):
    return lax.dot_general(x, y, (((1,), (0,)), ((), ())), preferred_element_type=jnp.float32)


def mm_nt(x, y):
    return lax.dot_general(x, y, (((1,), (1,)), ((), ())), preferred_element_type=jnp.float32)


def mm_tn(x, y):
    return lax.dot_general(x, y, (((0,), (0,)), ((), ())), preferred_element_type=jnp.float32)


def halves(x):
    high = bf(x)
    return high, bf(x - high.astype(jnp.float32))


def sum_right(x, ones):
    high, low = halves(x)
    return mm(high, ones) + mm(low, ones)


def logistic(x):
    return 1.0 / (1.0 + jnp.exp(-x))


def flag(cond):
    return jnp.where(cond, 1.0, 0.0)


def iota(shape, dim):
    return lax.broadcasted_iota(jnp.int32, shape, dim)


def pair_blocks():
    return flag((iota((PAIR, PAIR), 0) < HEAD_DIM) == (iota((PAIR, PAIR), 1) < HEAD_DIM))


def scan_kernel(
    group,
    r_ref,
    k_ref,
    v_ref,
    d_ref,
    a_ref,
    d_off_ref,
    a_off_ref,
    extra_ref,
    out_ref,
    reach_ref,
    ends_ref,
    chain_ref,
):
    positions, width = r_ref.shape
    pairs = width // PAIR
    C = HEAD_DIM
    rows_per = group * C
    own_block = pair_blocks()
    own_bf = bf(own_block)
    row, col = iota((C, PAIR), 0), iota((C, PAIR), 1) & (HEAD_DIM - 1)
    strict, upto = row > col, row >= col
    eye = flag(row == col)
    first = iota((1, PAIR), 1) < HEAD_DIM
    tri = bf(flag(iota((C, C), 0) >= iota((C, C), 1)))
    level_masks = []
    for s in range(6):
        inside = (
            ((row >> (s + 1)) == (col >> (s + 1)))
            & (((row >> s) & 1) == 1)
            & (((col >> s) & 1) == 0)
        )
        level_masks.append(bf(flag(inside)))

    def spread(x):
        return jnp.concatenate([x, x], axis=0) * own_bf

    square = (iota((PAIR, PAIR), 0) == iota((PAIR, PAIR), 1)).astype(jnp.float32)
    for p in range(pairs):
        chain_ref[p, :PAIR] = jnp.zeros((PAIR, PAIR), jnp.float32)
        chain_ref[p, PAIR:] = square

    def step(g, carry):
        base = pl.multiple_of(g * rows_per, rows_per)
        rows = pl.ds(base, rows_per)
        items = []
        for p in range(pairs):
            lanes = slice(p * PAIR, (p + 1) * PAIR)
            k = k_ref[rows, lanes].astype(jnp.float32)
            u = k * lax.rsqrt(sum_right(k * k, own_bf) + key_eps)
            rem = u * logistic(a_ref[rows, lanes].astype(jnp.float32) + a_off_ref[:, lanes])
            e = extra_ref[rows, :]
            extra = jnp.where(first, e[:, 2 * p : 2 * p + 1], e[:, 2 * p + 1 : 2 * p + 2])
            lg = extra - HALF_EXP * logistic(
                d_ref[rows, lanes].astype(jnp.float32) + d_off_ref[:, lanes]
            )
            r = r_ref[rows, lanes].astype(jnp.float32)
            v = v_ref[rows, lanes]
            for c in range(group):
                cut = slice(c * C, (c + 1) * C)
                items.append((p, c, k[cut], u[cut], rem[cut], lg[cut], r[cut], v[cut]))
        stage = []
        for p, c, k, u, rem, lg, r, v in items:
            high, low = halves(lg)
            rest = bf(lg - high.astype(jnp.float32) - low.astype(jnp.float32))
            cumul = mm(tri, high) + mm(tri, low) + mm(tri, rest)
            stage.append(cumul)
        work = []
        for (p, c, k, u, rem, lg, r, v), cumul in zip(items, stage):
            mid = 0.5 * cumul[C - 1 : C]
            up_now, down = jnp.exp(cumul - mid), jnp.exp(mid - cumul)
            up_before = jnp.exp(cumul - lg - mid)
            half = jnp.exp(mid)
            cq, cu, dk, dr = r * up_now, u * up_before, k * down, rem * down
            left = bf(jnp.concatenate([cu, cq], axis=0))
            pair_r = mm_nt(left, spread(bf(dr)))
            pair_k = mm_nt(left, spread(bf(dk)))
            work.append((cq * half, bf(cu * half), bf(dk * half), bf(dr * half), half * half, pair_r, pair_k))
        solve = []
        for (p, c, k, u, rem, lg, r, v), (qe, ue, kt, rt, ed, pair_r, pair_k) in zip(items, work):
            rp = bf(jnp.where(strict, pair_r[:C], 0.0))
            rr = bf(jnp.where(upto, pair_r[C:], 0.0))
            kp = jnp.where(strict, pair_k[:C], 0.0)
            rk = jnp.where(upto, pair_k[C:], 0.0)
            kv = mm(bf(jnp.concatenate([kp, rk], axis=0)), spread(v))
            inv = eye - (rp * level_masks[0]).astype(jnp.float32)
            solve.append([rp, rr, kv, inv])
        for s in range(1, 6):
            mids = [bf(mm(bf(inv), spread(rp * level_masks[s]))) for rp, rr, kv, inv in solve]
            for item, y in zip(solve, mids):
                item[3] = item[3] - mm(y, spread(bf(item[3])))
        wvs = []
        for (rp, rr, kv, inv), w in zip(solve, work):
            wide = jnp.concatenate([spread(w[1]), spread(bf(kv[:C]))], axis=1)
            wvs.append(bf(mm(bf(inv), wide)))
        tails = []
        for (rp, rr, kv, inv), (qe, ue, kt, rt, ed, _, _), wv, item in zip(solve, work, wvs, items):
            wide = jnp.concatenate([spread(wv[:, :PAIR]), spread(wv[:, PAIR:])], axis=1)
            rw = mm(rr, wide)
            read = bf(qe - rw[:, :PAIR])
            local = kv[C:] - rw[:, PAIR:]
            v = item[7]
            x = jnp.concatenate(
                [jnp.concatenate([v, jnp.zeros_like(v)], axis=1),
                 jnp.concatenate([-wv[:, PAIR:], -wv[:, :PAIR]], axis=1)], axis=0)
            nb = mm_tn(x, jnp.concatenate([kt, rt], axis=0))
            tails.append((read, local, nb[:PAIR] * own_block, bf(nb[PAIR:] * own_block), ed))
        z = [chain_ref[p] for p in range(pairs)]
        for c in range(group):
            for p in range(pairs):
                read, local, add, neg, ed = tails[p * group + c]
                zb = bf(z[p])
                qz = mm_nt(read, zb)
                at = pl.ds(pl.multiple_of(base + c * C, C), C)
                lanes = slice(p * PAIR, (p + 1) * PAIR)
                out_ref[at, lanes] = local + qz[:, :PAIR]
                reach_ref[at, lanes] = bf(qz[:, PAIR:])
                moved = z[p] * ed + mm(zb, neg)
                z[p] = jnp.concatenate([moved[:PAIR] + add, moved[PAIR:]], axis=0)
        for p in range(pairs):
            chain_ref[p] = z[p]
        return carry

    lax.fori_loop(0, positions // rows_per, step, 0)
    for p in range(pairs):
        s, m = chain_ref[p, :PAIR], chain_ref[p, PAIR:]
        ends_ref[p * 2 * C : p * 2 * C + C] = bf(s[:C] + s[C:])
        ends_ref[p * 2 * C + C : (p + 1) * 2 * C] = bf(m[:C] + m[C:])


def join_kernel(axis, all_ref, out_ref, reach_ref, gate_ref, gain_ref, mixed_ref):
    devices, place = lax.axis_size(axis), lax.axis_index(axis)
    width = out_ref.shape[1]
    pairs = width // PAIR
    C = HEAD_DIM
    own_block = pair_blocks()
    own_bf = bf(own_block)
    mean_bf = bf(own_block * (1.0 / HEAD_DIM))
    states = [jnp.zeros((C, PAIR), jnp.float32) for _ in range(pairs)]

    def hop(j, states):
        new = []
        for p in range(pairs):
            s = all_ref[j, p * 2 * C : p * 2 * C + C].astype(jnp.float32)
            m = all_ref[j, p * 2 * C + C : (p + 1) * 2 * C]
            m = jnp.concatenate([m, m], axis=0) * own_bf
            new.append(sum_right(states[p], m) + s)
        return tuple(new)

    states = lax.fori_loop(0, place, hop, tuple(states))
    for p in range(pairs):
        lanes = slice(p * PAIR, (p + 1) * PAIR)
        s = bf(states[p])
        s = jnp.concatenate([s, s], axis=0) * own_bf
        head = out_ref[:, lanes] + mm_nt(reach_ref[:, lanes], s)
        centred = head - sum_right(head, mean_bf)
        spread = sum_right(centred * centred, mean_bf)
        normed = centred * lax.rsqrt(spread + group_eps)
        gate = logistic(gate_ref[:, lanes].astype(jnp.float32))
        mixed_ref[:, lanes] = bf(normed * gain_ref[:, lanes] * gate)


def place_of():
    n_ep, n_tp = lax.axis_size("ep"), lax.axis_size("tp")
    e, t = lax.axis_index("ep"), lax.axis_index("tp")
    core = lax.rem(t, 2)
    return n_ep, n_tp, n_tp // 2, e, t, lax.div(t, 2), core


def remote(src, dst, send, recv, e, t):
    return pltpu.make_async_remote_copy(
        src_ref=src,
        dst_ref=dst,
        send_sem=send,
        recv_sem=recv,
        device_id=(e, t),
        device_id_type=pl.DeviceIdType.MESH,
    )


def meet():
    n_ep, n_tp, n_y, e, t, y, core = place_of()
    barrier = pltpu.get_barrier_semaphore()

    def greet(pe, pt):
        pl.semaphore_signal(
            barrier, inc=1, device_id=(pe, pt), device_id_type=pl.DeviceIdType.MESH
        )

    for d in range(1, n_ep):
        greet(lax.rem(e + d, n_ep), t)
    greet(e, 2 * y + 1 - core)
    for d in range(1, n_y):
        greet(e, 2 * lax.rem(y + d, n_y) + core)
    pl.semaphore_wait(barrier, n_ep - 1 + n_y)


def dispatch_kernel(
    group,
    r_ref,
    k_ref,
    v_ref,
    d_ref,
    a_ref,
    d_off_ref,
    a_off_ref,
    extra_ref,
    cols_ref,
    out_ref,
    reach_ref,
    piece_ref,
    every_ref,
    chain_ref,
    ends_ref,
    own_sem,
    es,
    er,
    zs,
    zr,
    gs,
    gr,
    cs,
    cr,
    ys,
    yr,
    fs,
    fr,
):
    n_ep, n_tp, n_y, e, t, y, core = place_of()
    share = cols_ref.shape[2]
    other = 2 * y + 1 - core

    def columns(index):
        return pl.ds(pl.multiple_of(index * share, share), share)

    def block(source, index):
        return piece_ref.at[source, :, columns(index)]

    meet()
    own = pltpu.make_async_copy(cols_ref.at[e], block(e, t), own_sem.at[0])
    own_ends = pltpu.make_async_copy(ends_ref, every_ref.at[e], own_sem.at[1])
    own.start()

    def ep_copy(d):
        peer = lax.rem(e + d, n_ep)
        return remote(cols_ref.at[peer], block(e, t), es.at[d], er.at[d], peer, t)

    n_x = gs.shape[0]
    n_z = n_ep // n_x
    z, x = lax.div(e, n_x), lax.rem(e, n_x)

    def up_copy(zz):
        ref = every_ref.at[zz * n_x + x]
        return remote(ref, ref, zs.at[zz], zr.at[zz], e + n_x, t)

    def side_copy(zz, h):
        ref = every_ref.at[zz * n_x + x]
        peer = z * n_x + lax.rem(x + h, n_x)
        return remote(ref, ref, gs.at[h, zz], gr.at[h, zz], peer, t)

    def pass_ends(zz):
        @pl.when(z + 1 < n_z)
        def _():
            up_copy(zz).start()

        for h in range(1, n_x):
            side_copy(zz, h).start()

    def relay_ends(i):
        @pl.when(z >= i)
        def _():
            up_copy(z - i).wait_recv()
            pass_ends(z - i)

    def close_ends(zz):
        @pl.when(z >= zz)
        def _():
            @pl.when(z + 1 < n_z)
            def _():
                up_copy(zz).wait_send()

            for h in range(1, n_x):
                side_copy(zz, h).wait()

    def source(d):
        return lax.rem(e - d + n_ep, n_ep)

    def core_copy(d):
        return remote(block(source(d), t), block(source(d), t), cs.at[d], cr.at[d], e, other)

    def y_copy(d, h):
        peer = 2 * lax.rem(y + h, n_y) + core
        return remote(block(source(d), t), block(source(d), t), ys.at[h, d], yr.at[h, d], e, peer)

    def forward_copy(d, h):
        index = 2 * lax.rem(y - h + n_y, n_y) + core
        return remote(
            block(source(d), index), block(source(d), index), fs.at[h, d], fr.at[h, d], e, other
        )

    def every(first, body, last=n_ep):
        def run(d, carry):
            body(d)
            return carry

        lax.fori_loop(first, last, run, 0)

    every(1, lambda d: ep_copy(d).start())

    def share_out(d):
        core_copy(d).start()
        for h in range(1, n_y):
            y_copy(d, h).start()

    own.wait()
    share_out(0)
    scan_kernel(
        group,
        r_ref,
        k_ref,
        v_ref,
        d_ref,
        a_ref,
        d_off_ref,
        a_off_ref,
        extra_ref,
        out_ref,
        reach_ref,
        ends_ref,
        chain_ref,
    )

    def arrived(d):
        ep_copy(d).wait_recv()
        share_out(d)

    own_ends.start()
    own_ends.wait()
    pass_ends(z)
    every(1, arrived)
    every(1, relay_ends, n_z)

    def pass_on(d):
        for h in range(1, n_y):
            y_copy(d, h).wait_recv()
            forward_copy(d, h).start()

    every(0, pass_on)

    def close(d):
        core_copy(d).wait()
        for h in range(1, n_y):
            y_copy(d, h).wait_send()
            forward_copy(d, h).wait()

    every(0, close)

    def close_far(d):
        ep_copy(d).wait_send()

    every(1, close_far)
    every(0, close_ends, n_z)


def return_kernel(
    piece_ref,
    every_ref,
    local_ref,
    reach_ref,
    gate_in_ref,
    gain_ref,
    out_weight_ref,
    gate_hbm,
    up_hbm,
    down_hbm,
    home_ref,
    mixer_ref,
    mixed_ref,
    proj_ref,
    gate_ref,
    up_ref,
    down_ref,
    rows_ref,
    hidden_ref,
    part_ref,
    near_ref,
    stage_ref,
    far_ref,
    final_ref,
    mnear_ref,
    mstage_ref,
    mfar_ref,
    gate_sem,
    up_sem,
    down_sem,
    ns,
    nr,
    ys,
    yr,
    es,
    er,
    mns,
    mnr,
    mys,
    myr,
):
    n_ep, n_tp, n_y, e, t, y, core = place_of()
    capacity, model = part_ref.shape[1:]
    units = gate_ref.shape[1]
    share = model // n_tp
    rows = proj_ref.shape[0] // (2 * n_tp)
    other = 2 * y + 1 - core
    half = n_ep // 2
    wide_units, wide_model = min(256, units), min(512, model)

    def gate_copy(i):
        at = pl.ds(pl.multiple_of(i * wide_units, wide_units), wide_units)
        return (
            pltpu.make_async_copy(gate_hbm.at[0, :, at], gate_ref.at[:, at], gate_sem.at[i]),
            pltpu.make_async_copy(up_hbm.at[0, :, at], up_ref.at[:, at], up_sem.at[i]),
        )

    def down_copy(i):
        at = pl.ds(pl.multiple_of(i * wide_model, wide_model), wide_model)
        return pltpu.make_async_copy(down_hbm.at[0, :, at], down_ref.at[:, at], down_sem.at[i])

    for i in range(units // wide_units):
        for copy in gate_copy(i):
            copy.start()
    for i in range(model // wide_model):
        down_copy(i).start()

    def columns(index):
        return pl.ds(pl.multiple_of(index * share, share), share)

    def row_block(index, q):
        return pl.ds(pl.multiple_of((2 * index + q) * rows, rows), rows)

    def peer_y(h):
        return lax.rem(y + h, n_y)

    def near_copy(s, h):
        src = part_ref.at[s, :, columns(2 * peer_y(h) + 1 - core)]
        return remote(src, near_ref.at[s, h], ns.at[s, h], nr.at[s, h], e, other)

    def y_copy(s, h):
        return remote(
            stage_ref.at[s, h], far_ref.at[s, h], ys.at[s, h], yr.at[s, h], e, 2 * peer_y(h) + core
        )

    def offset(k):
        m = lax.div(k + 1, 2)
        return lax.rem(half + m * (2 * lax.rem(k, 2) - 1) + n_ep, n_ep)

    def home_of(k):
        return lax.rem(e + offset(k), n_ep)

    def home_copy(k):
        peer, d = home_of(k), offset(k)
        return remote(final_ref.at[peer], home_ref.at[e], es.at[d], er.at[d], peer, t)

    def mnear_copy(q, h):
        src = proj_ref.at[row_block(2 * peer_y(h) + 1 - core, q), :]
        return remote(src, mnear_ref.at[q, h], mns.at[q, h], mnr.at[q, h], e, other)

    def my_copy(q, h):
        target = 2 * peer_y(h) + core
        return remote(
            mstage_ref.at[q, h], mfar_ref.at[q, h], mys.at[q, h], myr.at[q, h], e, target
        )

    def span(first, last, body):
        def run(d, carry):
            body(d)
            return carry

        lax.fori_loop(first, last, run, 0)

    def wide(x):
        return x.astype(jnp.float32)

    def mixer_sum(q, h):
        return wide(proj_ref[row_block(2 * peer_y(h) + core, q), :]) + wide(mnear_ref[q, h])

    def mixer_share(q):
        for h in range(1, n_y):
            mnear_copy(q, h).wait_recv()
            mstage_ref[q, h] = bf(mixer_sum(q, h))
            my_copy(q, h).start()

    def mixer_end(q):
        mnear_copy(q, 0).wait_recv()
        total = mixer_sum(q, 0)
        for h in range(1, n_y):
            my_copy(q, h).wait_recv()
            total = total + wide(mfar_ref[q, h])
        mixer_ref[q * rows : (q + 1) * rows] = bf(total)

    def widen(b):
        def take(k):
            at = pl.ds(pl.multiple_of((k - b * half) * capacity, capacity), capacity)
            rows_ref[at, :] = piece_ref[home_of(k)]

        span(b * half, (b + 1) * half, take)

        def unit_tile(i):
            if b == 0:
                for copy in gate_copy(i):
                    copy.wait()
            at = pl.ds(pl.multiple_of(i * wide_units, wide_units), wide_units)
            x = rows_ref[...]
            gate_val = mm(x, gate_ref[:, at])
            hidden_ref[:, at] = bf(gate_val * logistic(gate_val) * mm(x, up_ref[:, at]))

        span(0, units // wide_units, unit_tile)

    def narrow(b):
        def model_tile(i):
            if b == 0:
                down_copy(i).wait()
            at = pl.ds(pl.multiple_of(i * wide_model, wide_model), wide_model)
            result = bf(mm(hidden_ref[...], down_ref[:, at]))
            for j in range(half):
                part_ref[home_of(b * half + j), :, at] = result[j * capacity : (j + 1) * capacity]

        span(0, model // wide_model, model_tile)

    def start_near(k):
        for h in range(n_y):
            near_copy(home_of(k), h).start()

    def pair_sum(s, h):
        return wide(part_ref[s, :, columns(2 * peer_y(h) + core)]) + wide(near_ref[s, h])

    def add_near(k):
        s = home_of(k)
        for h in range(1, n_y):
            near_copy(s, h).wait_recv()
            stage_ref[s, h] = bf(pair_sum(s, h))
            y_copy(s, h).start()

    def add_far(s):
        near_copy(s, 0).wait_recv()
        total = pair_sum(s, 0)
        for h in range(1, n_y):
            y_copy(s, h).wait_recv()
            total = total + wide(far_ref[s, h])
        return bf(total)

    def go_home(k):
        s = home_of(k)
        final_ref[s] = add_far(s)
        home_copy(k).start()

    join_kernel("ep", every_ref, local_ref, reach_ref, gate_in_ref, gain_ref, mixed_ref)

    def project(i):
        at = pl.ds(pl.multiple_of(i * wide_model, wide_model), wide_model)
        proj_ref[:, at] = bf(mm(mixed_ref[...], out_weight_ref[:, at]))

    span(0, model // wide_model, project)
    meet()
    for q in range(2):
        for h in range(n_y):
            mnear_copy(q, h).start()
    mixer_share(0)
    widen(0)
    narrow(0)
    span(0, half, start_near)
    widen(1)
    span(0, half, add_near)
    narrow(1)
    span(half, n_ep, start_near)
    span(half, n_ep, add_near)
    mixer_share(1)
    span(0, half, go_home)
    mixer_end(0)
    span(half, n_ep - 1, go_home)
    home_ref[e] = add_far(e)
    mixer_end(1)

    def close(s):
        for h in range(n_y):
            near_copy(s, h).wait_send()
        for h in range(1, n_y):
            y_copy(s, h).wait_send()

    span(0, n_ep, close)
    for q in range(2):
        for h in range(n_y):
            mnear_copy(q, h).wait_send()
        for h in range(1, n_y):
            my_copy(q, h).wait_send()
    span(0, n_ep - 1, lambda k: home_copy(k).wait())


def experts_and_back(
    piece, everyone, local, reach, gate_input, gain, out_weight, gate_weight, up_weight, down_weight
):
    n_ep, n_tp = lax.axis_size("ep"), lax.axis_size("tp")
    n_y = n_tp // 2
    capacity, model = piece.shape[1:]
    units = gate_weight.shape[2]
    share, rows = model // n_tp, local.shape[0] // n_tp
    width = local.shape[1]
    out_weight = jnp.pad(out_weight, ((0, width - out_weight.shape[0]), (0, 0)))
    many, few = pltpu.SemaphoreType.DMA((n_ep, n_y)), pltpu.SemaphoreType.DMA((2, n_y))
    one = pltpu.SemaphoreType.DMA((n_ep,))

    def held(*shape):
        return pltpu.VMEM(shape, jnp.bfloat16)

    in_vmem = pl.BlockSpec(memory_space=pltpu.VMEM)
    return pl.pallas_call(
        return_kernel,
        out_shape=(
            jax.ShapeDtypeStruct((n_ep, capacity, share), jnp.bfloat16),
            jax.ShapeDtypeStruct((rows, model), jnp.bfloat16),
        ),
        in_specs=[in_vmem] * 7 + [pl.BlockSpec(memory_space=pltpu.HBM)] * 3,
        out_specs=[in_vmem] * 2,
        scratch_shapes=[
            held(*local.shape),
            held(local.shape[0], model),
            held(model, units),
            held(model, units),
            held(units, model),
            held(n_ep // 2 * capacity, model),
            held(n_ep // 2 * capacity, units),
            held(n_ep, capacity, model),
        ]
        + [held(n_ep, n_y, capacity, share)] * 3
        + [held(n_ep, capacity, share)]
        + [held(2, n_y, rows // 2, model)] * 3
        + [pltpu.SemaphoreType.DMA((max(1, units // 256),))] * 2
        + [pltpu.SemaphoreType.DMA((max(1, model // 512),))]
        + [many] * 4
        + [one] * 2
        + [few] * 4,
        compiler_params=pltpu.CompilerParams(
            collective_id=1, has_side_effects=True, vmem_limit_bytes=BACK_LIMIT
        ),
    )(
        piece,
        everyone,
        local,
        reach,
        gate_input,
        gain,
        out_weight,
        gate_weight,
        up_weight,
        down_weight,
    )


def scan_and_dispatch(
    own_columns,
    receptance,
    key_matrix,
    value_matrix,
    decay_data_term,
    correction_rate_data,
    output_gate_input,
    decay_channel_offset,
    correction_rate_offset,
    extra_head_log_decay,
    head_norm_gain,
):
    positions, own_width = receptance.shape
    pairs = -(-own_width // PAIR)
    width = pairs * PAIR

    def filled(x, columns=width):
        return x if x.shape[-1] == columns else jnp.pad(x, ((0, 0), (0, columns - x.shape[-1])))

    blocks = positions // HEAD_DIM
    group = 4 if blocks % 4 == 0 else 1
    n_ep, n_tp = lax.axis_size("ep"), lax.axis_size("tp")
    n_y = n_tp // 2
    n_x = 1
    while 4 * n_x * n_x <= n_ep:
        n_x = 2 * n_x
    capacity, share = own_columns.shape[1:]
    ends = (pairs * 2 * HEAD_DIM, PAIR)
    one, many = pltpu.SemaphoreType.DMA((n_ep,)), pltpu.SemaphoreType.DMA((n_y, n_ep))
    local, reach, piece, everyone = pl.pallas_call(
        functools.partial(dispatch_kernel, group),
        out_shape=(
            jax.ShapeDtypeStruct((positions, width), jnp.float32),
            jax.ShapeDtypeStruct((positions, width), jnp.bfloat16),
            jax.ShapeDtypeStruct((n_ep, capacity, n_tp * share), jnp.bfloat16),
            jax.ShapeDtypeStruct((n_ep, *ends), jnp.bfloat16),
        ),
        in_specs=[pl.BlockSpec(memory_space=pltpu.VMEM)] * 9,
        out_specs=[pl.BlockSpec(memory_space=pltpu.VMEM)] * 4,
        scratch_shapes=[
            pltpu.VMEM((pairs, 2 * PAIR, PAIR), jnp.float32),
            pltpu.VMEM(ends, jnp.bfloat16),
            pltpu.SemaphoreType.DMA((2,)),
        ]
        + [one] * 2
        + [pltpu.SemaphoreType.DMA((n_ep // n_x,))] * 2
        + [pltpu.SemaphoreType.DMA((n_x, n_ep // n_x))] * 2
        + [one] * 2
        + [many] * 4,
        compiler_params=pltpu.CompilerParams(
            collective_id=0, has_side_effects=True, vmem_limit_bytes=16 << 20
        ),
    )(
        filled(receptance),
        filled(key_matrix),
        filled(value_matrix),
        filled(decay_data_term),
        filled(correction_rate_data),
        filled(decay_channel_offset[None]),
        filled(correction_rate_offset[None]),
        filled(extra_head_log_decay, 2 * pairs),
        own_columns,
    )
    gate_input, gain = filled(output_gate_input), filled(head_norm_gain[None])
    return local, reach, piece, everyone, gate_input, gain


def expert_route(
    expert_layer_input,
    feedforward_norm_gain,
    group_router_weight,
    expert_router_weight,
    routes,
):
    token_rows = expert_layer_input.shape[0]
    route_count = routes.shape[1]
    ep_count = lax.axis_size("ep")
    expert_total = expert_router_weight.shape[1]
    per_group = expert_total // GROUPS
    capacity = 4 * token_rows // ep_count
    widened = expert_layer_input.astype(jnp.float32)
    normed_input = (
        widened
        * lax.rsqrt(jnp.mean(widened * widened, axis=-1, keepdims=True) + norm_eps)
        * feedforward_norm_gain
    ).astype(jnp.bfloat16)
    group_logit = jnp.dot(normed_input, group_router_weight, preferred_element_type=jnp.float32)
    group_exp = jnp.exp(group_logit)
    group_prob = group_exp / jnp.sum(group_exp, axis=-1, keepdims=True)
    expert_logit = jnp.dot(normed_input, expert_router_weight, preferred_element_type=jnp.float32)
    expert_range = jnp.arange(expert_total, dtype=jnp.int32)
    matched = routes[:, :, None] == expert_range[None, None, :]
    chosen_logit = jnp.sum(jnp.where(matched, expert_logit[:, None, :], 0.0), axis=-1)
    group_match = (routes // per_group)[:, :, None] == jnp.arange(GROUPS, dtype=jnp.int32)[
        None, None, :
    ]
    chosen_group = jnp.sum(jnp.where(group_match, group_prob[:, None, :], 0.0), axis=-1)
    route_weight = chosen_group * jax.nn.sigmoid(chosen_logit - chosen_logit[:, ::-1])
    flat_match = matched.reshape(token_rows * route_count, expert_total).astype(jnp.int32)
    before = jnp.cumsum(flat_match, axis=0) - flat_match
    placed = jnp.sum(before * flat_match, axis=1)
    slot_ids = routes.reshape(-1) * capacity + placed
    slot_range = jnp.arange(expert_total * capacity, dtype=jnp.int32)
    struck = (slot_range[:, None] == slot_ids[None, :]).reshape(
        expert_total * capacity, token_rows, route_count
    )
    dispatch_matrix = jnp.any(struck, axis=-1).astype(jnp.bfloat16)
    combine_matrix = jnp.sum(jnp.where(struck, route_weight[None, :, :], 0.0), axis=-1)
    outgoing = jnp.dot(dispatch_matrix, normed_input, preferred_element_type=jnp.float32).astype(
        jnp.bfloat16
    )
    outgoing = outgoing.reshape(ep_count, capacity, outgoing.shape[1])
    width_share = outgoing.shape[2] // lax.axis_size("tp")
    own_columns = lax.dynamic_slice_in_dim(
        outgoing, lax.axis_index("tp") * width_share, width_share, 2
    )
    return own_columns, combine_matrix


def expert_combine(homebound, combine_matrix):
    homebound = homebound.reshape(-1, homebound.shape[2]).astype(jnp.float32)
    combined = lax.dot_general(
        combine_matrix, homebound, (((0,), (0,)), ((), ())), precision=highest
    )
    return combined.astype(jnp.bfloat16)


def local(
    receptance,
    key_matrix,
    value_matrix,
    decay_data_term,
    correction_rate_data,
    output_gate_input,
    decay_channel_offset,
    correction_rate_offset,
    extra_head_log_decay,
    head_norm_gain,
    mixer_output_weight,
    expert_layer_input,
    feedforward_norm_gain,
    group_router_weight,
    expert_router_weight,
    routes,
    expert_gate_weight,
    expert_up_weight,
    expert_down_weight,
):
    own_columns, combine_matrix = expert_route(
        expert_layer_input,
        feedforward_norm_gain,
        group_router_weight,
        expert_router_weight,
        routes,
    )
    local_read, reach, piece, everyone, gate_input, gain = scan_and_dispatch(
        own_columns,
        receptance,
        key_matrix,
        value_matrix,
        decay_data_term,
        correction_rate_data,
        output_gate_input,
        decay_channel_offset,
        correction_rate_offset,
        extra_head_log_decay,
        head_norm_gain,
    )
    homebound, token_mixer_output = experts_and_back(
        piece,
        everyone,
        local_read,
        reach,
        gate_input,
        gain,
        mixer_output_weight,
        expert_gate_weight,
        expert_up_weight,
        expert_down_weight,
    )
    return (token_mixer_output, expert_combine(homebound, combine_matrix))


def solution(mesh):
    in_specs = (
        P("ep", "tp"),
        P("ep", "tp"),
        P("ep", "tp"),
        P("ep", "tp"),
        P("ep", "tp"),
        P("ep", "tp"),
        P("tp"),
        P("tp"),
        P("ep", "tp"),
        P("tp"),
        P("tp", None),
        P("ep", None),
        P(),
        P(),
        P(),
        P("ep", None),
        P("ep", None, "tp"),
        P("ep", None, "tp"),
        P("ep", "tp", None),
    )
    out_specs = (P(("ep", "tp"), None), P("ep", "tp"))
    return jax.shard_map(local, mesh=mesh, in_specs=in_specs, out_specs=out_specs, check_vma=False)
```

```python
import functools
import math

import jax
import jax.numpy as jnp
from jax import lax
from jax.experimental import pallas as pl
from jax.experimental.pallas import tpu as pltpu
from jax.sharding import PartitionSpec as P

HEAD_DIM = 64
PAIR = 2 * HEAD_DIM
BACK_LIMIT = 32 << 20
HALF_EXP = math.exp(-0.5)
GROUPS = 4


key_eps = 1e-06
group_eps = 0.00064
norm_eps = 1e-06
highest = lax.Precision.HIGHEST


def bf(x):
    return x.astype(jnp.bfloat16)


def mm(x, y):
    return lax.dot_general(x, y, (((1,), (0,)), ((), ())), preferred_element_type=jnp.float32)


def mm_nt(x, y):
    return lax.dot_general(x, y, (((1,), (1,)), ((), ())), preferred_element_type=jnp.float32)


def mm_tn(x, y):
    return lax.dot_general(x, y, (((0,), (0,)), ((), ())), preferred_element_type=jnp.float32)


def halves(x):
    high = bf(x)
    return high, bf(x - high.astype(jnp.float32))


def sum_right(x, ones):
    high, low = halves(x)
    return mm(high, ones) + mm(low, ones)


def logistic(x):
    return 1.0 / (1.0 + jnp.exp(-x))


def flag(cond):
    return jnp.where(cond, 1.0, 0.0)


def iota(shape, dim):
    return lax.broadcasted_iota(jnp.int32, shape, dim)


def pair_blocks():
    return flag((iota((PAIR, PAIR), 0) < HEAD_DIM) == (iota((PAIR, PAIR), 1) < HEAD_DIM))


def scan_kernel(
    group,
    r_ref,
    k_ref,
    v_ref,
    d_ref,
    a_ref,
    d_off_ref,
    a_off_ref,
    extra_ref,
    out_ref,
    reach_ref,
    ends_ref,
    chain_ref,
):
    positions, width = r_ref.shape
    pairs = width // PAIR
    C = HEAD_DIM
    rows_per = group * C
    own_block = pair_blocks()
    own_bf = bf(own_block)
    row, col = iota((C, PAIR), 0), iota((C, PAIR), 1) & (HEAD_DIM - 1)
    strict, upto = row > col, row >= col
    eye = flag(row == col)
    first = iota((1, PAIR), 1) < HEAD_DIM
    tri = bf(flag(iota((C, C), 0) >= iota((C, C), 1)))
    level_masks = []
    for s in range(6):
        inside = (
            ((row >> (s + 1)) == (col >> (s + 1)))
            & (((row >> s) & 1) == 1)
            & (((col >> s) & 1) == 0)
        )
        level_masks.append(bf(flag(inside)))

    def spread(x):
        return jnp.concatenate([x, x], axis=0) * own_bf

    square = (iota((PAIR, PAIR), 0) == iota((PAIR, PAIR), 1)).astype(jnp.float32)
    for p in range(pairs):
        chain_ref[p, :PAIR] = jnp.zeros((PAIR, PAIR), jnp.float32)
        chain_ref[p, PAIR:] = square

    def step(g, carry):
        base = pl.multiple_of(g * rows_per, rows_per)
        rows = pl.ds(base, rows_per)
        items = []
        for p in range(pairs):
            lanes = slice(p * PAIR, (p + 1) * PAIR)
            k = k_ref[rows, lanes].astype(jnp.float32)
            u = k * lax.rsqrt(sum_right(k * k, own_bf) + key_eps)
            rem = u * logistic(a_ref[rows, lanes].astype(jnp.float32) + a_off_ref[:, lanes])
            e = extra_ref[rows, :]
            extra = jnp.where(first, e[:, 2 * p : 2 * p + 1], e[:, 2 * p + 1 : 2 * p + 2])
            lg = extra - HALF_EXP * logistic(
                d_ref[rows, lanes].astype(jnp.float32) + d_off_ref[:, lanes]
            )
            r = r_ref[rows, lanes].astype(jnp.float32)
            v = v_ref[rows, lanes]
            for c in range(group):
                cut = slice(c * C, (c + 1) * C)
                items.append((p, c, k[cut], u[cut], rem[cut], lg[cut], r[cut], v[cut]))
        stage = []
        for p, c, k, u, rem, lg, r, v in items:
            high, low = halves(lg)
            rest = bf(lg - high.astype(jnp.float32) - low.astype(jnp.float32))
            cumul = mm(tri, high) + mm(tri, low) + mm(tri, rest)
            stage.append(cumul)
        work = []
        for (p, c, k, u, rem, lg, r, v), cumul in zip(items, stage):
            mid = 0.5 * cumul[C - 1 : C]
            up_now, down = jnp.exp(cumul - mid), jnp.exp(mid - cumul)
            up_before = jnp.exp(cumul - lg - mid)
            half = jnp.exp(mid)
            cq, cu, dk, dr = r * up_now, u * up_before, k * down, rem * down
            left = bf(jnp.concatenate([cu, cq], axis=0))
            pair_r = mm_nt(left, spread(bf(dr)))
            pair_k = mm_nt(left, spread(bf(dk)))
            work.append((cq * half, bf(cu * half), bf(dk * half), bf(dr * half), half * half, pair_r, pair_k))
        solve = []
        for (p, c, k, u, rem, lg, r, v), (qe, ue, kt, rt, ed, pair_r, pair_k) in zip(items, work):
            rp = bf(jnp.where(strict, pair_r[:C], 0.0))
            rr = bf(jnp.where(upto, pair_r[C:], 0.0))
            kp = jnp.where(strict, pair_k[:C], 0.0)
            rk = jnp.where(upto, pair_k[C:], 0.0)
            kv = mm(bf(jnp.concatenate([kp, rk], axis=0)), spread(v))
            inv = eye - (rp * level_masks[0]).astype(jnp.float32)
            solve.append([rp, rr, kv, inv])
        for s in range(1, 6):
            mids = [bf(mm(bf(inv), spread(rp * level_masks[s]))) for rp, rr, kv, inv in solve]
            for item, y in zip(solve, mids):
                item[3] = item[3] - mm(y, spread(bf(item[3])))
        wvs = []
        for (rp, rr, kv, inv), w in zip(solve, work):
            wide = jnp.concatenate([spread(w[1]), spread(bf(kv[:C]))], axis=1)
            wvs.append(bf(mm(bf(inv), wide)))
        tails = []
        for (rp, rr, kv, inv), (qe, ue, kt, rt, ed, _, _), wv, item in zip(solve, work, wvs, items):
            wide = jnp.concatenate([spread(wv[:, :PAIR]), spread(wv[:, PAIR:])], axis=1)
            rw = mm(rr, wide)
            read = bf(qe - rw[:, :PAIR])
            local = kv[C:] - rw[:, PAIR:]
            v = item[7]
            x = jnp.concatenate(
                [jnp.concatenate([v, jnp.zeros_like(v)], axis=1),
                 jnp.concatenate([-wv[:, PAIR:], -wv[:, :PAIR]], axis=1)], axis=0)
            nb = mm_tn(x, jnp.concatenate([kt, rt], axis=0))
            tails.append((read, local, nb[:PAIR] * own_block, bf(nb[PAIR:] * own_block), ed))
        z = [chain_ref[p] for p in range(pairs)]
        for c in range(group):
            for p in range(pairs):
                read, local, add, neg, ed = tails[p * group + c]
                zb = bf(z[p])
                qz = mm_nt(read, zb)
                at = pl.ds(pl.multiple_of(base + c * C, C), C)
                lanes = slice(p * PAIR, (p + 1) * PAIR)
                out_ref[at, lanes] = local + qz[:, :PAIR]
                reach_ref[at, lanes] = bf(qz[:, PAIR:])
                moved = z[p] * ed + mm(zb, neg)
                z[p] = jnp.concatenate([moved[:PAIR] + add, moved[PAIR:]], axis=0)
        for p in range(pairs):
            chain_ref[p] = z[p]
        return carry

    lax.fori_loop(0, positions // rows_per, step, 0)
    for p in range(pairs):
        s, m = chain_ref[p, :PAIR], chain_ref[p, PAIR:]
        ends_ref[p * 2 * C : p * 2 * C + C] = bf(s[:C] + s[C:])
        ends_ref[p * 2 * C + C : (p + 1) * 2 * C] = bf(m[:C] + m[C:])


def join_kernel(axis, all_ref, out_ref, reach_ref, gate_ref, gain_ref, mixed_ref):
    devices, place = lax.axis_size(axis), lax.axis_index(axis)
    width = out_ref.shape[1]
    pairs = width // PAIR
    C = HEAD_DIM
    own_block = pair_blocks()
    own_bf = bf(own_block)
    mean_bf = bf(own_block * (1.0 / HEAD_DIM))
    states = [jnp.zeros((C, PAIR), jnp.float32) for _ in range(pairs)]

    def hop(j, states):
        new = []
        for p in range(pairs):
            s = all_ref[j, p * 2 * C : p * 2 * C + C].astype(jnp.float32)
            m = all_ref[j, p * 2 * C + C : (p + 1) * 2 * C]
            m = jnp.concatenate([m, m], axis=0) * own_bf
            new.append(sum_right(states[p], m) + s)
        return tuple(new)

    states = lax.fori_loop(0, place, hop, tuple(states))
    for p in range(pairs):
        lanes = slice(p * PAIR, (p + 1) * PAIR)
        s = bf(states[p])
        s = jnp.concatenate([s, s], axis=0) * own_bf
        head = out_ref[:, lanes] + mm_nt(reach_ref[:, lanes], s)
        centred = head - sum_right(head, mean_bf)
        spread = sum_right(centred * centred, mean_bf)
        normed = centred * lax.rsqrt(spread + group_eps)
        gate = logistic(gate_ref[:, lanes].astype(jnp.float32))
        mixed_ref[:, lanes] = bf(normed * gain_ref[:, lanes] * gate)


def place_of():
    n_ep, n_tp = lax.axis_size("ep"), lax.axis_size("tp")
    e, t = lax.axis_index("ep"), lax.axis_index("tp")
    core = lax.rem(t, 2)
    return n_ep, n_tp, n_tp // 2, e, t, lax.div(t, 2), core


def remote(src, dst, send, recv, e, t):
    return pltpu.make_async_remote_copy(
        src_ref=src,
        dst_ref=dst,
        send_sem=send,
        recv_sem=recv,
        device_id=(e, t),
        device_id_type=pl.DeviceIdType.MESH,
    )


def meet():
    n_ep, n_tp, n_y, e, t, y, core = place_of()
    barrier = pltpu.get_barrier_semaphore()

    def greet(pe, pt):
        pl.semaphore_signal(
            barrier, inc=1, device_id=(pe, pt), device_id_type=pl.DeviceIdType.MESH
        )

    for d in range(1, n_ep):
        greet(lax.rem(e + d, n_ep), t)
    greet(e, 2 * y + 1 - core)
    for d in range(1, n_y):
        greet(e, 2 * lax.rem(y + d, n_y) + core)
    pl.semaphore_wait(barrier, n_ep - 1 + n_y)


def dispatch_kernel(
    group,
    r_ref,
    k_ref,
    v_ref,
    d_ref,
    a_ref,
    d_off_ref,
    a_off_ref,
    extra_ref,
    cols_ref,
    out_ref,
    reach_ref,
    piece_ref,
    every_ref,
    chain_ref,
    ends_ref,
    own_sem,
    es,
    er,
    zs,
    zr,
    gs,
    gr,
    cs,
    cr,
    ys,
    yr,
    fs,
    fr,
):
    n_ep, n_tp, n_y, e, t, y, core = place_of()
    share = cols_ref.shape[2]
    other = 2 * y + 1 - core

    def columns(index):
        return pl.ds(pl.multiple_of(index * share, share), share)

    def block(source, index):
        return piece_ref.at[source, :, columns(index)]

    meet()
    own = pltpu.make_async_copy(cols_ref.at[e], block(e, t), own_sem.at[0])
    own_ends = pltpu.make_async_copy(ends_ref, every_ref.at[e], own_sem.at[1])
    own.start()

    def ep_copy(d):
        peer = lax.rem(e + d, n_ep)
        return remote(cols_ref.at[peer], block(e, t), es.at[d], er.at[d], peer, t)

    n_x = gs.shape[0]
    n_z = n_ep // n_x
    z, x = lax.div(e, n_x), lax.rem(e, n_x)

    def up_copy(zz):
        ref = every_ref.at[zz * n_x + x]
        return remote(ref, ref, zs.at[zz], zr.at[zz], e + n_x, t)

    def side_copy(zz, h):
        ref = every_ref.at[zz * n_x + x]
        peer = z * n_x + lax.rem(x + h, n_x)
        return remote(ref, ref, gs.at[h, zz], gr.at[h, zz], peer, t)

    def pass_ends(zz):
        @pl.when(z + 1 < n_z)
        def _():
            up_copy(zz).start()

        for h in range(1, n_x):
            side_copy(zz, h).start()

    def relay_ends(i):
        @pl.when(z >= i)
        def _():
            up_copy(z - i).wait_recv()
            pass_ends(z - i)

    def close_ends(zz):
        @pl.when(z >= zz)
        def _():
            @pl.when(z + 1 < n_z)
            def _():
                up_copy(zz).wait_send()

            for h in range(1, n_x):
                side_copy(zz, h).wait()

    def source(d):
        return lax.rem(e - d + n_ep, n_ep)

    def core_copy(d):
        return remote(block(source(d), t), block(source(d), t), cs.at[d], cr.at[d], e, other)

    def y_copy(d, h):
        peer = 2 * lax.rem(y + h, n_y) + core
        return remote(block(source(d), t), block(source(d), t), ys.at[h, d], yr.at[h, d], e, peer)

    def forward_copy(d, h):
        index = 2 * lax.rem(y - h + n_y, n_y) + core
        return remote(
            block(source(d), index), block(source(d), index), fs.at[h, d], fr.at[h, d], e, other
        )

    def every(first, body, last=n_ep):
        def run(d, carry):
            body(d)
            return carry

        lax.fori_loop(first, last, run, 0)

    every(1, lambda d: ep_copy(d).start())

    def share_out(d):
        core_copy(d).start()
        for h in range(1, n_y):
            y_copy(d, h).start()

    own.wait()
    share_out(0)
    scan_kernel(
        group,
        r_ref,
        k_ref,
        v_ref,
        d_ref,
        a_ref,
        d_off_ref,
        a_off_ref,
        extra_ref,
        out_ref,
        reach_ref,
        ends_ref,
        chain_ref,
    )

    def arrived(d):
        ep_copy(d).wait_recv()
        share_out(d)

    own_ends.start()
    own_ends.wait()
    pass_ends(z)
    every(1, arrived)
    every(1, relay_ends, n_z)

    def pass_on(d):
        for h in range(1, n_y):
            y_copy(d, h).wait_recv()
            forward_copy(d, h).start()

    every(0, pass_on)

    def close(d):
        core_copy(d).wait()
        for h in range(1, n_y):
            y_copy(d, h).wait_send()
            forward_copy(d, h).wait()

    every(0, close)

    def close_far(d):
        ep_copy(d).wait_send()

    every(1, close_far)
    every(0, close_ends, n_z)


def return_kernel(
    piece_ref,
    every_ref,
    local_ref,
    reach_ref,
    gate_in_ref,
    gain_ref,
    out_weight_ref,
    gate_hbm,
    up_hbm,
    down_hbm,
    home_ref,
    mixer_ref,
    mixed_ref,
    proj_ref,
    gate_ref,
    up_ref,
    down_ref,
    rows_ref,
    hidden_ref,
    part_ref,
    near_ref,
    stage_ref,
    far_ref,
    final_ref,
    mnear_ref,
    mstage_ref,
    mfar_ref,
    gate_sem,
    up_sem,
    down_sem,
    ns,
    nr,
    ys,
    yr,
    es,
    er,
    mns,
    mnr,
    mys,
    myr,
):
    n_ep, n_tp, n_y, e, t, y, core = place_of()
    capacity, model = part_ref.shape[1:]
    units = gate_ref.shape[1]
    share = model // n_tp
    rows = proj_ref.shape[0] // (2 * n_tp)
    other = 2 * y + 1 - core
    half = n_ep // 2
    wide_units, wide_model = min(256, units), min(512, model)

    def gate_copy(i):
        at = pl.ds(pl.multiple_of(i * wide_units, wide_units), wide_units)
        return (
            pltpu.make_async_copy(gate_hbm.at[0, :, at], gate_ref.at[:, at], gate_sem.at[i]),
            pltpu.make_async_copy(up_hbm.at[0, :, at], up_ref.at[:, at], up_sem.at[i]),
        )

    def down_copy(i):
        at = pl.ds(pl.multiple_of(i * wide_model, wide_model), wide_model)
        return pltpu.make_async_copy(down_hbm.at[0, :, at], down_ref.at[:, at], down_sem.at[i])

    for i in range(units // wide_units):
        for copy in gate_copy(i):
            copy.start()
    for i in range(model // wide_model):
        down_copy(i).start()

    def columns(index):
        return pl.ds(pl.multiple_of(index * share, share), share)

    def row_block(index, q):
        return pl.ds(pl.multiple_of((2 * index + q) * rows, rows), rows)

    def peer_y(h):
        return lax.rem(y + h, n_y)

    def near_copy(s, h):
        src = part_ref.at[s, :, columns(2 * peer_y(h) + 1 - core)]
        return remote(src, near_ref.at[s, h], ns.at[s, h], nr.at[s, h], e, other)

    def y_copy(s, h):
        return remote(
            stage_ref.at[s, h], far_ref.at[s, h], ys.at[s, h], yr.at[s, h], e, 2 * peer_y(h) + core
        )

    def offset(k):
        m = lax.div(k + 1, 2)
        return lax.rem(half + m * (2 * lax.rem(k, 2) - 1) + n_ep, n_ep)

    def home_of(k):
        return lax.rem(e + offset(k), n_ep)

    def home_copy(k):
        peer, d = home_of(k), offset(k)
        return remote(final_ref.at[peer], home_ref.at[e], es.at[d], er.at[d], peer, t)

    def mnear_copy(q, h):
        src = proj_ref.at[row_block(2 * peer_y(h) + 1 - core, q), :]
        return remote(src, mnear_ref.at[q, h], mns.at[q, h], mnr.at[q, h], e, other)

    def my_copy(q, h):
        target = 2 * peer_y(h) + core
        return remote(
            mstage_ref.at[q, h], mfar_ref.at[q, h], mys.at[q, h], myr.at[q, h], e, target
        )

    def span(first, last, body):
        def run(d, carry):
            body(d)
            return carry

        lax.fori_loop(first, last, run, 0)

    def wide(x):
        return x.astype(jnp.float32)

    def mixer_sum(q, h):
        return wide(proj_ref[row_block(2 * peer_y(h) + core, q), :]) + wide(mnear_ref[q, h])

    def mixer_share(q):
        for h in range(1, n_y):
            mnear_copy(q, h).wait_recv()
            mstage_ref[q, h] = bf(mixer_sum(q, h))
            my_copy(q, h).start()

    def mixer_end(q):
        mnear_copy(q, 0).wait_recv()
        total = mixer_sum(q, 0)
        for h in range(1, n_y):
            my_copy(q, h).wait_recv()
            total = total + wide(mfar_ref[q, h])
        mixer_ref[q * rows : (q + 1) * rows] = bf(total)

    def widen(b):
        def take(k):
            at = pl.ds(pl.multiple_of((k - b * half) * capacity, capacity), capacity)
            rows_ref[at, :] = piece_ref[home_of(k)]

        span(b * half, (b + 1) * half, take)

        def unit_tile(i):
            if b == 0:
                for copy in gate_copy(i):
                    copy.wait()
            at = pl.ds(pl.multiple_of(i * wide_units, wide_units), wide_units)
            x = rows_ref[...]
            gate_val = mm(x, gate_ref[:, at])
            hidden_ref[:, at] = bf(gate_val * logistic(gate_val) * mm(x, up_ref[:, at]))

        span(0, units // wide_units, unit_tile)

    def narrow(b):
        def model_tile(i):
            if b == 0:
                down_copy(i).wait()
            at = pl.ds(pl.multiple_of(i * wide_model, wide_model), wide_model)
            result = bf(mm(hidden_ref[...], down_ref[:, at]))
            for j in range(half):
                part_ref[home_of(b * half + j), :, at] = result[j * capacity : (j + 1) * capacity]

        span(0, model // wide_model, model_tile)

    def start_near(k):
        for h in range(n_y):
            near_copy(home_of(k), h).start()

    def pair_sum(s, h):
        return wide(part_ref[s, :, columns(2 * peer_y(h) + core)]) + wide(near_ref[s, h])

    def add_near(k):
        s = home_of(k)
        for h in range(1, n_y):
            near_copy(s, h).wait_recv()
            stage_ref[s, h] = bf(pair_sum(s, h))
            y_copy(s, h).start()

    def add_far(s):
        near_copy(s, 0).wait_recv()
        total = pair_sum(s, 0)
        for h in range(1, n_y):
            y_copy(s, h).wait_recv()
            total = total + wide(far_ref[s, h])
        return bf(total)

    def go_home(k):
        s = home_of(k)
        final_ref[s] = add_far(s)
        home_copy(k).start()

    join_kernel("ep", every_ref, local_ref, reach_ref, gate_in_ref, gain_ref, mixed_ref)

    def project(i):
        at = pl.ds(pl.multiple_of(i * wide_model, wide_model), wide_model)
        proj_ref[:, at] = bf(mm(mixed_ref[...], out_weight_ref[:, at]))

    span(0, model // wide_model, project)
    meet()
    for q in range(2):
        for h in range(n_y):
            mnear_copy(q, h).start()
    mixer_share(0)
    widen(0)
    narrow(0)
    span(0, half, start_near)
    widen(1)
    span(0, half, add_near)
    narrow(1)
    span(half, n_ep, start_near)
    span(half, n_ep, add_near)
    mixer_share(1)
    span(0, half, go_home)
    mixer_end(0)
    span(half, n_ep - 1, go_home)
    home_ref[e] = add_far(e)
    mixer_end(1)

    def close(s):
        for h in range(n_y):
            near_copy(s, h).wait_send()
        for h in range(1, n_y):
            y_copy(s, h).wait_send()

    span(0, n_ep, close)
    for q in range(2):
        for h in range(n_y):
            mnear_copy(q, h).wait_send()
        for h in range(1, n_y):
            my_copy(q, h).wait_send()
    span(0, n_ep - 1, lambda k: home_copy(k).wait())


def experts_and_back(
    piece, everyone, local, reach, gate_input, gain, out_weight, gate_weight, up_weight, down_weight
):
    n_ep, n_tp = lax.axis_size("ep"), lax.axis_size("tp")
    n_y = n_tp // 2
    capacity, model = piece.shape[1:]
    units = gate_weight.shape[2]
    share, rows = model // n_tp, local.shape[0] // n_tp
    width = local.shape[1]
    out_weight = jnp.pad(out_weight, ((0, width - out_weight.shape[0]), (0, 0)))
    many, few = pltpu.SemaphoreType.DMA((n_ep, n_y)), pltpu.SemaphoreType.DMA((2, n_y))
    one = pltpu.SemaphoreType.DMA((n_ep,))

    def held(*shape):
        return pltpu.VMEM(shape, jnp.bfloat16)

    in_vmem = pl.BlockSpec(memory_space=pltpu.VMEM)
    return pl.pallas_call(
        return_kernel,
        out_shape=(
            jax.ShapeDtypeStruct((n_ep, capacity, share), jnp.bfloat16),
            jax.ShapeDtypeStruct((rows, model), jnp.bfloat16),
        ),
        in_specs=[in_vmem] * 7 + [pl.BlockSpec(memory_space=pltpu.HBM)] * 3,
        out_specs=[in_vmem] * 2,
        scratch_shapes=[
            held(*local.shape),
            held(local.shape[0], model),
            held(model, units),
            held(model, units),
            held(units, model),
            held(n_ep // 2 * capacity, model),
            held(n_ep // 2 * capacity, units),
            held(n_ep, capacity, model),
        ]
        + [held(n_ep, n_y, capacity, share)] * 3
        + [held(n_ep, capacity, share)]
        + [held(2, n_y, rows // 2, model)] * 3
        + [pltpu.SemaphoreType.DMA((max(1, units // 256),))] * 2
        + [pltpu.SemaphoreType.DMA((max(1, model // 512),))]
        + [many] * 4
        + [one] * 2
        + [few] * 4,
        compiler_params=pltpu.CompilerParams(
            collective_id=1, has_side_effects=True, vmem_limit_bytes=BACK_LIMIT
        ),
    )(
        piece,
        everyone,
        local,
        reach,
        gate_input,
        gain,
        out_weight,
        gate_weight,
        up_weight,
        down_weight,
    )


def scan_and_dispatch(
    own_columns,
    receptance,
    key_matrix,
    value_matrix,
    decay_data_term,
    correction_rate_data,
    output_gate_input,
    decay_channel_offset,
    correction_rate_offset,
    extra_head_log_decay,
    head_norm_gain,
):
    positions, own_width = receptance.shape
    pairs = -(-own_width // PAIR)
    width = pairs * PAIR

    def filled(x, columns=width):
        return x if x.shape[-1] == columns else jnp.pad(x, ((0, 0), (0, columns - x.shape[-1])))

    blocks = positions // HEAD_DIM
    group = 4 if blocks % 4 == 0 else 1
    n_ep, n_tp = lax.axis_size("ep"), lax.axis_size("tp")
    n_y = n_tp // 2
    n_x = 1
    while 4 * n_x * n_x <= n_ep:
        n_x = 2 * n_x
    capacity, share = own_columns.shape[1:]
    ends = (pairs * 2 * HEAD_DIM, PAIR)
    one, many = pltpu.SemaphoreType.DMA((n_ep,)), pltpu.SemaphoreType.DMA((n_y, n_ep))
    local, reach, piece, everyone = pl.pallas_call(
        functools.partial(dispatch_kernel, group),
        out_shape=(
            jax.ShapeDtypeStruct((positions, width), jnp.float32),
            jax.ShapeDtypeStruct((positions, width), jnp.bfloat16),
            jax.ShapeDtypeStruct((n_ep, capacity, n_tp * share), jnp.bfloat16),
            jax.ShapeDtypeStruct((n_ep, *ends), jnp.bfloat16),
        ),
        in_specs=[pl.BlockSpec(memory_space=pltpu.VMEM)] * 9,
        out_specs=[pl.BlockSpec(memory_space=pltpu.VMEM)] * 4,
        scratch_shapes=[
            pltpu.VMEM((pairs, 2 * PAIR, PAIR), jnp.float32),
            pltpu.VMEM(ends, jnp.bfloat16),
            pltpu.SemaphoreType.DMA((2,)),
        ]
        + [one] * 2
        + [pltpu.SemaphoreType.DMA((n_ep // n_x,))] * 2
        + [pltpu.SemaphoreType.DMA((n_x, n_ep // n_x))] * 2
        + [one] * 2
        + [many] * 4,
        compiler_params=pltpu.CompilerParams(
            collective_id=0, has_side_effects=True, vmem_limit_bytes=16 << 20
        ),
        cost_estimate=pl.CostEstimate(
            flops=200000 * positions * width,
            bytes_accessed=16 * positions * width,
            transcendentals=0,
        ),
    )(
        filled(receptance),
        filled(key_matrix),
        filled(value_matrix),
        filled(decay_data_term),
        filled(correction_rate_data),
        filled(decay_channel_offset[None]),
        filled(correction_rate_offset[None]),
        filled(extra_head_log_decay, 2 * pairs),
        own_columns,
    )
    gate_input, gain = filled(output_gate_input), filled(head_norm_gain[None])
    return local, reach, piece, everyone, gate_input, gain


def expert_route(
    expert_layer_input,
    feedforward_norm_gain,
    group_router_weight,
    expert_router_weight,
    routes,
):
    token_rows = expert_layer_input.shape[0]
    route_count = routes.shape[1]
    ep_count = lax.axis_size("ep")
    expert_total = expert_router_weight.shape[1]
    per_group = expert_total // GROUPS
    capacity = 4 * token_rows // ep_count
    widened = expert_layer_input.astype(jnp.float32)
    normed_input = (
        widened
        * lax.rsqrt(jnp.mean(widened * widened, axis=-1, keepdims=True) + norm_eps)
        * feedforward_norm_gain
    ).astype(jnp.bfloat16)
    group_logit = jnp.dot(normed_input, group_router_weight, preferred_element_type=jnp.float32)
    group_exp = jnp.exp(group_logit)
    group_prob = group_exp / jnp.sum(group_exp, axis=-1, keepdims=True)
    expert_logit = jnp.dot(normed_input, expert_router_weight, preferred_element_type=jnp.float32)
    expert_range = jnp.arange(expert_total, dtype=jnp.int32)
    matched = routes[:, :, None] == expert_range[None, None, :]
    chosen_logit = jnp.sum(jnp.where(matched, expert_logit[:, None, :], 0.0), axis=-1)
    group_match = (routes // per_group)[:, :, None] == jnp.arange(GROUPS, dtype=jnp.int32)[
        None, None, :
    ]
    chosen_group = jnp.sum(jnp.where(group_match, group_prob[:, None, :], 0.0), axis=-1)
    route_weight = chosen_group * jax.nn.sigmoid(chosen_logit - chosen_logit[:, ::-1])
    flat_match = matched.reshape(token_rows * route_count, expert_total).astype(jnp.int32)
    before = jnp.cumsum(flat_match, axis=0) - flat_match
    placed = jnp.sum(before * flat_match, axis=1)
    slot_ids = routes.reshape(-1) * capacity + placed
    slot_range = jnp.arange(expert_total * capacity, dtype=jnp.int32)
    struck = (slot_range[:, None] == slot_ids[None, :]).reshape(
        expert_total * capacity, token_rows, route_count
    )
    dispatch_matrix = jnp.any(struck, axis=-1).astype(jnp.bfloat16)
    combine_matrix = jnp.sum(jnp.where(struck, route_weight[None, :, :], 0.0), axis=-1)
    outgoing = jnp.dot(dispatch_matrix, normed_input, preferred_element_type=jnp.float32).astype(
        jnp.bfloat16
    )
    outgoing = outgoing.reshape(ep_count, capacity, outgoing.shape[1])
    width_share = outgoing.shape[2] // lax.axis_size("tp")
    own_columns = lax.dynamic_slice_in_dim(
        outgoing, lax.axis_index("tp") * width_share, width_share, 2
    )
    return own_columns, combine_matrix


def expert_combine(homebound, combine_matrix):
    homebound = homebound.reshape(-1, homebound.shape[2]).astype(jnp.float32)
    combined = lax.dot_general(
        combine_matrix, homebound, (((0,), (0,)), ((), ())), precision=highest
    )
    return combined.astype(jnp.bfloat16)


def local(
    receptance,
    key_matrix,
    value_matrix,
    decay_data_term,
    correction_rate_data,
    output_gate_input,
    decay_channel_offset,
    correction_rate_offset,
    extra_head_log_decay,
    head_norm_gain,
    mixer_output_weight,
    expert_layer_input,
    feedforward_norm_gain,
    group_router_weight,
    expert_router_weight,
    routes,
    expert_gate_weight,
    expert_up_weight,
    expert_down_weight,
):
    own_columns, combine_matrix = expert_route(
        expert_layer_input,
        feedforward_norm_gain,
        group_router_weight,
        expert_router_weight,
        routes,
    )
    local_read, reach, piece, everyone, gate_input, gain = scan_and_dispatch(
        own_columns,
        receptance,
        key_matrix,
        value_matrix,
        decay_data_term,
        correction_rate_data,
        output_gate_input,
        decay_channel_offset,
        correction_rate_offset,
        extra_head_log_decay,
        head_norm_gain,
    )
    homebound, token_mixer_output = experts_and_back(
        piece,
        everyone,
        local_read,
        reach,
        gate_input,
        gain,
        mixer_output_weight,
        expert_gate_weight,
        expert_up_weight,
        expert_down_weight,
    )
    return (token_mixer_output, expert_combine(homebound, combine_matrix))


def solution(mesh):
    in_specs = (
        P("ep", "tp"),
        P("ep", "tp"),
        P("ep", "tp"),
        P("ep", "tp"),
        P("ep", "tp"),
        P("ep", "tp"),
        P("tp"),
        P("tp"),
        P("ep", "tp"),
        P("tp"),
        P("tp", None),
        P("ep", None),
        P(),
        P(),
        P(),
        P("ep", None),
        P("ep", None, "tp"),
        P("ep", None, "tp"),
        P("ep", "tp", None),
    )
    out_specs = (P(("ep", "tp"), None), P("ep", "tp"))
    return jax.shard_map(local, mesh=mesh, in_specs=in_specs, out_specs=out_specs, check_vma=False)
```
